32 devices in a mesh: grp: 2 (over x), ep: 4 (over y, core), tp: 4 (over z).
Axes of the slice: x: 2, y: 2, z: 4, core: 2. Of those that a mesh axis runs over, the one named last changes fastest.
Arguments:
- tokens: bfloat16 [2048, 4096], P(('grp', 'ep')), parts along dimension 0, may hold values from -6 to 6
- expert_ids: int32 [2048, 2], P(('grp', 'ep')), parts along dimension 0, may hold values from 0 to 15, as said below
- gates: float32 [2048, 2], P(('grp', 'ep')), parts along dimension 0, may hold values from 0.1 to 1
- w_gate: bfloat16 [16, 4096, 2048], P('ep', None, 'tp'), may hold values from -0.09375 to 0.09375
- w_up: bfloat16 [16, 4096, 2048], P('ep', None, 'tp'), may hold values from -0.09375 to 0.09375
- w_down: bfloat16 [16, 2048, 4096], P('ep', 'tp'), may hold values from -0.79549513 to 0.79549513, as said below
- norm_gain: float32 [4096], P('tp'), may hold values from 0.1 to 1.9
- norm_bias: float32 [4096], P('tp'), may hold values from -1.5 to 1.5
Outputs:
- normed: bfloat16 [2048, 4096], P(('grp', 'ep'), 'tp'), parts along dimension 0
The draws below stay inside these ranges and needn't reach their ends.
There are 2 independent parts, one for each index of `grp`. The reference program is written for one: setup_inputs(seed, part) draws one part's arguments, and reference() takes and returns one part's arrays. A program takes and returns all parts, laid end to end along the dimension named above; an argument that names none is the same for every part. Nothing has to cross between parts.
Inputs may be any that keep to these rules, and one draw needn't show every extreme that they name: `expert_ids`: each row names 2 different experts, both in the same group of 4 consecutive expert numbers. Within one aligned block of 256 rows no expert is named more than 64 times, and in every draw some expert is named exactly 64 times in every block. `w_down`: down projection weights.
All inputs are finite; a program needn't handle non-finite values.
Results may differ from the reference program's by a relative error of at most 0.014.
Values may be sent and summed in bfloat16 or wider, within the bound.
A program may use at most 128 MiB of HBM per device.

```python
import math
import jax
import jax.numpy as jnp
from jax import lax

D = 4096
FF = 2048
GROUPS = 4
EXPERTS_PER_GROUP = 4
TOPK = 2
TOK_DEV = 256
EXPERTS = 16
CAP = 64
SLOTS = 256
FF_DEV = 512
TOKENS = 1024
N_EP = 4
N_TP = 4


def route_block(block_key, busy_group):
    key_weights, key_labels, key_shuffle = jax.random.split(block_key, 3)
    weights = jax.random.randint(key_weights, (GROUPS,), 4, 9)
    is_busy = jnp.arange(GROUPS) == busy_group
    weights = jnp.where(is_busy, 0, weights)
    busy_count = TOK_DEV // 2
    remainder = TOK_DEV - busy_count
    counts = remainder * weights // jnp.sum(weights)
    leftover = remainder - jnp.sum(counts)
    first_other = jnp.argmin(is_busy.astype(jnp.int32))
    counts = counts + leftover * (jnp.arange(GROUPS) == first_other).astype(jnp.int32)
    counts = jnp.where(is_busy, busy_count, counts)
    group_ends = jnp.cumsum(counts)
    group_starts = group_ends - counts
    position = jnp.arange(TOK_DEV)
    group_of = jnp.sum((position[:, None] >= group_ends[None, :]).astype(jnp.int32), axis=1)
    within = position - group_starts[group_of]
    first_table = jnp.array([0, 2, 0, 1, 0, 1], jnp.int32)
    second_table = jnp.array([1, 3, 2, 3, 3, 2], jnp.int32)
    relabel = jax.vmap(lambda label_key: jax.random.permutation(label_key, EXPERTS_PER_GROUP))(jax.random.split(key_labels, GROUPS))
    group_base = group_of * EXPERTS_PER_GROUP
    first_expert = group_base + relabel[group_of, first_table[within % 6]]
    second_expert = group_base + relabel[group_of, second_table[within % 6]]
    chosen = jnp.stack([first_expert, second_expert], axis=1).astype(jnp.int32)
    shuffle = jax.random.permutation(key_shuffle, TOK_DEV)
    return chosen[shuffle]


def draw_expert_ids(key, part):
    busy_group = jax.random.randint(jax.random.fold_in(key, 7), (), 0, GROUPS)
    block_keys = jax.random.split(jax.random.fold_in(key, 11), TOKENS // TOK_DEV)
    chosen = jax.vmap(route_block, in_axes=(0, None))(block_keys, busy_group)
    return chosen.reshape(TOKENS, TOPK).astype(jnp.int32)


def draw_w_down(key, part):
    noise = jnp.clip(jax.random.normal(jax.random.fold_in(key, 3), (EXPERTS, FF, D), jnp.float32), -6.0, 6.0)
    columns = 0.6 * jnp.exp(math.log(3.0) * jnp.arange(D, dtype=jnp.float32) / (D - 1))
    return (noise * FF ** (-0.5) * columns).astype(jnp.bfloat16)


def shard_levels(key, extent, shards, low, top_value):
    gain = 1.0
    for dim, shards_of in shards:
        draws = jax.random.uniform(jax.random.fold_in(jax.random.fold_in(key, 6), dim), (shards_of,), jnp.float32, low / len(shards), top_value / len(shards))
        gain = gain * jnp.repeat(jnp.exp(draws), extent[dim] // shards_of).reshape((-1,) + (1,) * (len(extent) - 1 - dim))
    return gain


def normal_values(key, shape, width, limit, cuts=(), kind=jnp.bfloat16):
    drawn = width * jax.random.normal(key, shape, jnp.float32)
    if cuts:
        drawn = drawn * shard_levels(key, shape, cuts, -0.22, 0.18)
    return jnp.clip(drawn, -limit, limit).astype(kind)


def setup_inputs(seed: int = 0, part: int = 0) -> dict:
    seeds = jax.random.split(jax.random.key(seed), 9)
    part_splits = jax.random.split(jax.random.fold_in(seeds[8], part), 9)
    tokens = normal_values(part_splits[0], (TOKENS, D), 1.0, 6.0, ((0, 4),))
    expert_ids = draw_expert_ids(jax.random.fold_in(jax.random.fold_in(seeds[8], part), 71), part)
    gates = jnp.clip(0.1 + 0.9 * jax.random.uniform(part_splits[2], (TOKENS, TOPK), jnp.float32) ** shard_levels(part_splits[2], (TOKENS, TOPK), ((0, 4),), -0.2, 0.2), 0.1, 1.0)
    w_gate = normal_values(seeds[3], (EXPERTS, D, FF), D ** -0.5, 0.09375, ((0, 4), (2, 4)))
    w_up = normal_values(seeds[4], (EXPERTS, D, FF), D ** -0.5, 0.09375, ((0, 4), (2, 4)))
    w_down = draw_w_down(jax.random.fold_in(seeds[8], 71), part)
    norm_gain = jnp.clip(1.0 + 0.18 * jax.random.normal(seeds[6], (D,), jnp.float32), 0.1, 1.9)
    norm_bias = normal_values(seeds[7], (D,), 0.3, 1.5, ((0, 4),), jnp.float32)
    return dict(tokens=tokens, expert_ids=expert_ids, gates=gates, w_gate=w_gate, w_up=w_up, w_down=w_down, norm_gain=norm_gain, norm_bias=norm_bias)


norm_eps = 1e-05

def run_expert(operands):
    routed, gate_w, up_w, down_w = operands
    gate_part = jnp.dot(routed, gate_w, preferred_element_type=jnp.float32)
    up_part = jnp.dot(routed, up_w, preferred_element_type=jnp.float32)
    hidden = (jax.nn.silu(gate_part) * up_part).astype(jnp.bfloat16)
    blocks = hidden.reshape(SLOTS, N_TP, FF_DEV).astype(jnp.float32)
    down_blocks = down_w.reshape(N_TP, FF_DEV, D).astype(jnp.float32)
    partial_value = jnp.einsum('rjf,jfd->jrd', blocks, down_blocks).astype(jnp.bfloat16)
    partial_value = lax.optimization_barrier(partial_value)
    return lax.optimization_barrier(jnp.sum(partial_value.astype(jnp.float32), axis=0)).astype(jnp.bfloat16)

def reference(tokens, expert_ids, gates, w_gate, w_up, w_down, norm_gain, norm_bias):
    flat_ids = expert_ids.reshape(N_EP, TOK_DEV * TOPK)
    onehot = (flat_ids[:, :, None] == jnp.arange(EXPERTS, dtype=jnp.int32)[None, None, :]).astype(jnp.int32)
    position = lax.optimization_barrier(jnp.sum((jnp.cumsum(onehot, axis=1) - 1) * onehot, axis=2))
    source_block = jnp.arange(N_EP, dtype=jnp.int32)[:, None]
    target = (flat_ids * SLOTS + source_block * CAP + position).reshape(-1).astype(jnp.int32)
    token_of = jnp.arange(TOKENS * TOPK, dtype=jnp.int32) // TOPK
    source = jnp.zeros((EXPERTS * SLOTS,), jnp.int32).at[target].set(token_of)
    filled = jnp.zeros((EXPERTS * SLOTS,), jnp.bool_).at[target].set(True)
    routed = jnp.where(filled[:, None], tokens[source], jnp.zeros((), jnp.bfloat16)).reshape(EXPERTS, SLOTS, D)
    expert_out = lax.map(run_expert, (routed, w_gate, w_up, w_down))
    picked = expert_out.reshape(EXPERTS * SLOTS, D)[target].reshape(TOKENS, TOPK, D)
    combined = lax.optimization_barrier(jnp.sum(picked.astype(jnp.float32) * gates[:, :, None], axis=1))
    row_mean = lax.optimization_barrier(jnp.mean(combined, axis=1, keepdims=True))
    centred = combined - row_mean
    row_var = lax.optimization_barrier(jnp.mean(centred * centred, axis=1, keepdims=True))
    normed = centred * lax.rsqrt(row_var + norm_eps) * norm_gain + norm_bias
    return normed.astype(jnp.bfloat16)
```

```python
import functools
import jax
import jax.numpy as jnp
from jax import lax
from jax.experimental import pallas as pl
from jax.experimental.pallas import tpu as pltpu
from jax.sharding import PartitionSpec as P

D = 4096
TOPK = 2
EXPERTS = 16
CAP = 64


norm_eps = 1e-05


def route_slots(expert_ids):
    flat_ids = expert_ids.reshape(-1)
    onehot = (flat_ids[:, None] == jnp.arange(EXPERTS, dtype=jnp.int32)[None, :]).astype(jnp.int32)
    position = jnp.sum((jnp.cumsum(onehot, axis=0) - 1) * onehot, axis=1)
    target = flat_ids * CAP + position
    token_of = jnp.arange(flat_ids.shape[0], dtype=jnp.int32) // TOPK
    source = jnp.zeros((EXPERTS * CAP,), jnp.int32).at[target].set(token_of)
    filled = jnp.zeros((EXPERTS * CAP,), jnp.bool_).at[target].set(True)
    return (target, source, filled)


def on_device(tokens, expert_ids, gates, w_gate, w_up, w_down, norm_gain, norm_bias):
    tok_rows, width = tokens.shape
    piece_width = norm_gain.shape[0]
    target, source, filled = route_slots(expert_ids)
    outgoing = jnp.where(filled[:, None], tokens[source], jnp.zeros((), jnp.bfloat16)).reshape(
        EXPERTS, CAP, width
    )
    arrived = lax.all_to_all(outgoing, "ep", split_axis=0, concat_axis=1, tiled=True)
    gate_part = jnp.einsum("erd,edf->erf", arrived, w_gate, preferred_element_type=jnp.float32)
    up_part = jnp.einsum("erd,edf->erf", arrived, w_up, preferred_element_type=jnp.float32)
    hidden = (jax.nn.silu(gate_part) * up_part).astype(jnp.bfloat16)
    partial_value = jnp.einsum("erf,efd->erd", hidden, w_down, preferred_element_type=jnp.float32)
    summed = lax.psum_scatter(
        partial_value.astype(jnp.bfloat16), "tp", scatter_dimension=2, tiled=True
    )
    returned = lax.all_to_all(summed, "ep", split_axis=1, concat_axis=0, tiled=True)
    picked = returned.reshape(EXPERTS * CAP, piece_width)[target].reshape(
        tok_rows, TOPK, piece_width
    )
    combined = jnp.sum(picked.astype(jnp.float32) * gates[:, :, None], axis=1)
    stats = lax.psum((jnp.sum(combined, axis=1), jnp.sum(combined * combined, axis=1)), "tp")
    row_mean = stats[0] / D
    row_var = stats[1] / D - row_mean * row_mean
    normed = (combined - row_mean[:, None]) * lax.rsqrt(
        row_var[:, None] + norm_eps
    ) * norm_gain + norm_bias
    return normed.astype(jnp.bfloat16)


GROUP_EXPERTS = 4
CHUNKS = 16
HALF = CHUNKS // 2
PASSES = 2
SLOTS = 3
PIECES = 8
SENT = 6
EARLY = 6
F32 = jnp.float32
BF16 = jnp.bfloat16
MESH = pl.DeviceIdType.MESH


def moe_kernel(
    ids_ref, gates_ref, gain_ref, bias_ref, tokens_ref, wg_ref, wu_ref, wd_ref,
    out_ref,
    tok, wbuf, wd, acc, hid, xr, dnb, place, collect, rowg, meta, meta_in,
    part, core_in, y_in, z_in, st_out, st_in,
    tok_sem, y_send, y_recv, z_send, z_recv, own_send, own_recv, fwd_send, fwd_recv,
    meta_send, meta_recv, w_sem, wd_sem, pc_send, pc_recv, py_send, py_recv,
    pz_send, pz_recv, st_send, st_recv,
):
    ep = lax.axis_index("ep")
    z = lax.axis_index("tp")
    y, c = ep // 2, ep % 2
    partner = y * 2 + (1 - c)
    across = (1 - y) * 2 + c
    diag = (1 - y) * 2 + (1 - c)
    par = z % 2
    zpeer = z + 1 - 2 * par
    rows, width = tokens_ref.shape
    band = rows // PASSES
    experts = wg_ref.shape[0]
    cols = width // CHUNKS
    piece = gain_ref.shape[1]
    part_cols = piece // 2

    def remote(src, dst, send, recv, e, t):
        return pltpu.make_async_remote_copy(
            src_ref=src, dst_ref=dst, send_sem=send, recv_sem=recv,
            device_id={"ep": e, "tp": t}, device_id_type=MESH,
        )

    def span(ch, size):
        return pl.ds(pl.multiple_of(ch * size, size), size)

    def load_tok(ch):
        return pltpu.make_async_copy(
            tokens_ref.at[:, span(ch, cols)], tok.at[ch, ep], tok_sem.at[ch])

    def band_rows(h):
        return pl.ds(h * band, band)

    def zshift(i):
        return (z + 3 - i // 2) % 4

    def load_wd(i):
        return pltpu.make_async_copy(
            wd_ref.at[:, :, span(zshift(i) * 2 + i % 2, part_cols)], wd.at[i], wd_sem.at[i])

    def direct(j):
        return par * HALF + j

    def swapped(j):
        return (1 - par) * HALF + j

    def load_unit(t):
        u, slot = t % HALF, t % SLOTS
        return [
            pltpu.make_async_copy(
                w_ref.at[:, span(ch, cols), :],
                wbuf.at[slot, g, :, pl.ds(k * cols, cols), :], w_sem.at[slot, g, k])
            for k, ch in enumerate((direct(u), swapped(u)))
            for g, w_ref in enumerate((wg_ref, wu_ref))
        ]

    def y_copy(h, j):
        blk = tok.at[direct(j), ep, band_rows(h)]
        return remote(blk, blk, y_send.at[h, j], y_recv.at[h, j], across, z)

    def y_arrive(h, j):
        blk = tok.at[direct(j), across, band_rows(h)]
        return remote(blk, blk, y_send.at[h, j], y_recv.at[h, j], across, z)

    def z_copy(h, j):
        blk = tok.at[direct(j), across, band_rows(h)]
        return remote(blk, blk, z_send.at[h, j], z_recv.at[h, j], ep, zpeer)

    def z_arrive(h, j):
        blk = tok.at[swapped(j), across, band_rows(h)]
        return remote(blk, blk, z_send.at[h, j], z_recv.at[h, j], ep, zpeer)

    def own_copy(h, ch):
        blk = tok.at[ch, ep, band_rows(h)]
        return remote(blk, blk, own_send.at[h, ch], own_recv.at[h, ch], partner, z)

    def own_arrive(h, ch):
        blk = tok.at[ch, partner, band_rows(h)]
        return remote(blk, blk, own_send.at[h, ch], own_recv.at[h, ch], partner, z)

    def fwd_copy(h, ch):
        blk = tok.at[ch, across, band_rows(h)]
        return remote(blk, blk, fwd_send.at[h, ch], fwd_recv.at[h, ch], partner, z)

    def fwd_arrive(h, ch):
        blk = tok.at[ch, diag, band_rows(h)]
        return remote(blk, blk, fwd_send.at[h, ch], fwd_recv.at[h, ch], partner, z)

    def meta_copy(e, k):
        return remote(meta.at[e], meta_in.at[ep], meta_send.at[k], meta_recv.at[k], e, z)

    def meta_arrive(e, k):
        return remote(meta.at[e], meta_in.at[e], meta_send.at[k], meta_recv.at[k], e, z)

    peers = (partner, across, diag)

    for j in range(HALF):
        load_tok(direct(j)).start()
    for j in range(HALF):
        load_tok(swapped(j)).start()
    for t in range(SLOTS):
        for cp in load_unit(t):
            cp.start()

    barrier = pltpu.get_barrier_semaphore()
    for e in peers:
        pl.semaphore_signal(barrier, inc=1, device_id={"ep": e, "tp": z}, device_id_type=MESH)
    for d in (1, 2, 3):
        pl.semaphore_signal(
            barrier, inc=1, device_id={"ep": ep, "tp": (z + d) % 4}, device_id_type=MESH)
    total_experts = 4 * experts
    expert_row = lax.broadcasted_iota(jnp.int32, (total_experts, rows), 0)
    first = ids_ref[0:1, :] == expert_row
    second = ids_ref[1:2, :] == expert_row
    named = jnp.where(first | second, 1.0, 0.0).astype(F32)
    weight = jnp.where(first, gates_ref[0:1, :], jnp.where(second, gates_ref[1:2, :], 0.0))
    tri_r = lax.broadcasted_iota(jnp.int32, (rows, rows), 0)
    tri_c = lax.broadcasted_iota(jnp.int32, (rows, rows), 1)
    before = jnp.where(
        (tri_r < tri_c) & (tri_r // band == tri_c // band), 1.0, 0.0).astype(BF16)
    position = jnp.dot(named.astype(BF16), before, preferred_element_type=F32)
    slot = jnp.where(
        named > 0.5, position + ((expert_row % experts) * CAP).astype(F32), -1.0)
    for e in range(4):
        meta[e, 0:experts, :] = slot[e * experts:(e + 1) * experts, :]
        meta[e, experts:2 * experts, :] = weight[e * experts:(e + 1) * experts, :]
    pl.semaphore_wait(barrier, 6)
    for k, e in enumerate(peers):
        meta_copy(e, k).start()

    for j in range(HALF):
        load_tok(direct(j)).wait()
        y_copy(0, j).start()
        own_copy(0, direct(j)).start()
    for j in range(HALF):
        load_tok(swapped(j)).wait()
        own_copy(0, swapped(j)).start()
    for j in range(HALF):
        y_copy(1, j).start()
    for ch in range(CHUNKS):
        own_copy(1, ch).start()
    for i in range(PIECES):
        load_wd(i).start()

    meta_in[ep] = meta[ep]
    acc[...] = jnp.zeros_like(acc)
    for k, e in enumerate(peers):
        meta_arrive(e, k).wait_recv()

    row_f = tri_r.astype(F32)
    for s in range(4):
        info = meta_in[s]
        put = jnp.zeros((rows, rows), F32)
        for e in range(experts):
            put += jnp.where(row_f == info[e:e + 1, :], 1.0, 0.0)
        back = put.T
        for h in range(PASSES):
            mine = slice(h * band, (h + 1) * band)
            place[h, s] = put[:, mine].astype(BF16)
            collect[h, s] = back[mine, :].astype(BF16)
            for e in range(experts):
                g = jnp.sum(
                    put[e * CAP:(e + 1) * CAP, mine]
                    * info[experts + e:experts + e + 1, mine],
                    axis=1, keepdims=True)
                rowg[h, e, s * CAP:(s + 1) * CAP, :] = jnp.broadcast_to(g, (CAP, 128))

    def unit(h, u):
        t = h * HALF + u
        for k, ch in enumerate((direct(u), swapped(u))):
            own_arrive(h, ch).wait_recv()
            fwd_arrive(h, ch).wait_recv()
            for s in range(4):
                x = jnp.dot(
                    place[h, s], tok[ch, s, band_rows(h), :],
                    preferred_element_type=F32).astype(BF16)
                for e in range(experts):
                    xr[e, s * CAP:(s + 1) * CAP, k * cols:(k + 1) * cols] = (
                        x[e * CAP:(e + 1) * CAP, :])
        for cp in load_unit(t):
            cp.wait()

        def one(e, carry):
            for g in range(2):
                acc[g, e] += jnp.dot(xr[e], wbuf[t % SLOTS, g, e], preferred_element_type=F32)
            return carry
        lax.fori_loop(0, experts, one, 0)

        @pl.when(t + SLOTS < PASSES * HALF)
        def _():
            for cp in load_unit(t + SLOTS):
                cp.start()

    def relay(h, j):
        @pl.when(j < HALF)
        def _():
            y_arrive(h, j).wait_recv()
            z_copy(h, j).start()
            fwd_copy(h, direct(j)).start()

        @pl.when((j >= 1) & (j <= HALF))
        def _():
            z_arrive(h, j - 1).wait_recv()
            fwd_copy(h, swapped(j - 1)).start()

    def activate(h):
        def one(e, carry):
            g = acc[0, e]
            v = g / (1.0 + jnp.exp(-g)) * acc[1, e]
            hid[e] = (v * rowg[h, e][:, 0:1]).astype(BF16)
            if h + 1 < PASSES:
                acc[0, e] = jnp.zeros_like(g)
                acc[1, e] = jnp.zeros_like(g)
            return carry
        lax.fori_loop(0, experts, one, 0)

    def core_copy(h, i):
        return remote(
            part.at[i, 1 - c, :, band_rows(h)], core_in.at[i, :, band_rows(h)],
            pc_send.at[h, i], pc_recv.at[h, i], partner, z)

    def ret_copy(h, i):
        return remote(
            part.at[i, c, 1 - y, band_rows(h)], y_in.at[i, band_rows(h)],
            py_send.at[h, i], py_recv.at[h, i], across, z)

    def scatter_copy(h, i):
        return remote(
            part.at[i, c, y, band_rows(h)], z_in.at[i, band_rows(h)],
            pz_send.at[h, i], pz_recv.at[h, i], ep, zshift(i))

    def down(h, i):
        if h == 0:
            load_wd(i).wait()

        def one(e, carry):
            o = jnp.dot(hid[e], wd[i, e], preferred_element_type=F32).astype(BF16)
            for s in range(4):
                dnb[s, span(e, CAP), :] = o[s * CAP:(s + 1) * CAP, :]
            return carry
        lax.fori_loop(0, experts, one, 0)

        def gather(s, carry):
            part[i, s % 2, s // 2, band_rows(h), :] = jnp.dot(
                collect[h, s], dnb[s], preferred_element_type=F32).astype(BF16)
            return carry
        lax.fori_loop(0, 4, gather, 0)
        core_copy(h, i).start()

    def give_back(h, i):
        core_copy(h, i).wait_recv()
        part[i, c, 1 - y, band_rows(h), :] += core_in[i, 1 - y, band_rows(h), :]
        ret_copy(h, i).start()

    def settle(h, k):
        ret_copy(h, k).wait_recv()
        part[k, c, y, band_rows(h), :] += (
            core_in[k, y, band_rows(h), :] + y_in[k, band_rows(h), :])

        @pl.when(k < SENT)
        def _():
            scatter_copy(h, k).start()

    def first_pass(j, carry):
        relay(0, j)

        @pl.when(j >= 2)
        def _():
            unit(0, j - 2)
        return carry
    lax.fori_loop(0, HALF + 2, first_pass, 0)
    activate(0)

    def second_pass(j, carry):
        relay(1, j)

        @pl.when((j >= 1) & (j <= PIECES))
        def _():
            give_back(0, j - 1)

        @pl.when(j < PIECES)
        def _():
            down(0, j)

        @pl.when(j >= 2)
        def _():
            unit(1, j - 2)

        @pl.when(j >= EARLY)
        def _():
            settle(0, j - EARLY)
        return carry
    lax.fori_loop(0, HALF + 2, second_pass, 0)
    activate(1)
    settled = HALF + 2 - EARLY

    def last_down(i, carry):
        @pl.when(i < PIECES)
        def _():
            down(1, i)

        @pl.when(i >= 1)
        def _():
            give_back(1, i - 1)

        @pl.when(i < PIECES - settled)
        def _():
            settle(0, i + settled)
        return carry
    lax.fori_loop(0, PIECES + 1, last_down, 0)

    def last_settle(k, carry):
        settle(1, k)
        return carry
    lax.fori_loop(0, PIECES, last_settle, 0)

    halves = []
    for n in range(2):
        half = part[SENT + n, c, y].astype(F32)
        for i in range(n, SENT, 2):
            for h in range(PASSES):
                scatter_copy(h, i).wait_recv()
            half += z_in[i].astype(F32)
        halves.append(half)
    total = jnp.concatenate(halves, axis=1)

    local_mean = jnp.sum(total, axis=1, keepdims=True) * (1.0 / piece)
    gap = total - local_mean
    local_m2 = jnp.sum(gap * gap, axis=1, keepdims=True)
    mean_t = jnp.broadcast_to(local_mean, (rows, 128)).T
    m2_t = jnp.broadcast_to(local_m2, (rows, 128)).T
    st_out[0:8, :] = mean_t[0:8, :]
    st_out[8:16, :] = m2_t[0:8, :]

    def stat_copy(d):
        return remote(
            st_out, st_in.at[d - 1], st_send.at[d - 1], st_recv.at[d - 1], ep, (z + d) % 4)
    for d in (1, 2, 3):
        stat_copy(d).start()
    for d in (1, 2, 3):
        stat_copy(d).wait_recv()
    means = [st_out[0:8, :]] + [st_in[d, 0:8, :] for d in range(3)]
    m2s = [st_out[8:16, :]] + [st_in[d, 8:16, :] for d in range(3)]
    mean = (means[0] + means[1] + means[2] + means[3]) * 0.25
    m2 = m2s[0] + m2s[1] + m2s[2] + m2s[3]
    for m in means:
        m2 += (m - mean) * (m - mean) * piece
    scale = lax.rsqrt(m2 * (1.0 / width) + norm_eps)
    mean_col = jnp.broadcast_to(mean[0:1, :], (128, rows)).T[:, 0:1]
    scale_col = jnp.broadcast_to(scale[0:1, :], (128, rows)).T[:, 0:1]
    out_ref[...] = (
        (total - mean_col) * scale_col * gain_ref[...] + bias_ref[...]).astype(BF16)

    def sent_tokens(j, carry):
        for h in range(PASSES):
            y_copy(h, j).wait_send()
            z_copy(h, j).wait_send()
            for ch in (direct(j), swapped(j)):
                own_copy(h, ch).wait_send()
                fwd_copy(h, ch).wait_send()
        return carry
    lax.fori_loop(0, HALF, sent_tokens, 0)
    for k, e in enumerate(peers):
        meta_copy(e, k).wait_send()
    for h in range(PASSES):
        for i in range(PIECES):
            core_copy(h, i).wait_send()
            ret_copy(h, i).wait_send()
        for i in range(SENT):
            scatter_copy(h, i).wait_send()
    for d in (1, 2, 3):
        stat_copy(d).wait_send()


def fused_on_device(tokens, expert_ids, gates, w_gate, w_up, w_down, norm_gain, norm_bias):
    rows, width = tokens.shape
    experts, _, hidden = w_gate.shape
    piece = norm_gain.shape[0]
    cols = width // CHUNKS
    part_cols = piece // 2
    band = rows // PASSES
    dma = pltpu.SemaphoreType.DMA
    vmem = pl.BlockSpec(memory_space=pltpu.VMEM)
    hbm = pl.BlockSpec(memory_space=pl.ANY)
    return pl.pallas_call(
        moe_kernel,
        out_shape=jax.ShapeDtypeStruct((rows, piece), jnp.bfloat16),
        in_specs=[vmem] * 4 + [hbm] * 4,
        out_specs=vmem,
        scratch_shapes=[
            pltpu.VMEM((CHUNKS, 4, rows, cols), BF16),
            pltpu.VMEM((SLOTS, 2, experts, 2 * cols, hidden), BF16),
            pltpu.VMEM((PIECES, experts, hidden, part_cols), BF16),
            pltpu.VMEM((2, experts, 4 * CAP, hidden), F32),
            pltpu.VMEM((experts, 4 * CAP, hidden), BF16),
            pltpu.VMEM((experts, 4 * CAP, 2 * cols), BF16),
            pltpu.VMEM((4, experts * CAP, part_cols), BF16),
            pltpu.VMEM((PASSES, 4, experts * CAP, band), BF16),
            pltpu.VMEM((PASSES, 4, band, experts * CAP), BF16),
            pltpu.VMEM((PASSES, experts, 4 * CAP, 128), F32),
            pltpu.VMEM((4, 2 * experts, rows), F32),
            pltpu.VMEM((4, 2 * experts, rows), F32),
            pltpu.VMEM((PIECES, 2, 2, rows, part_cols), BF16),
            pltpu.VMEM((PIECES, 2, rows, part_cols), BF16),
            pltpu.VMEM((PIECES, rows, part_cols), BF16),
            pltpu.VMEM((SENT, rows, part_cols), BF16),
            pltpu.VMEM((16, rows), F32),
            pltpu.VMEM((3, 16, rows), F32),
            dma((CHUNKS,)), dma((PASSES, HALF)), dma((PASSES, HALF)),
            dma((PASSES, HALF)), dma((PASSES, HALF)),
            dma((PASSES, CHUNKS)), dma((PASSES, CHUNKS)),
            dma((PASSES, CHUNKS)), dma((PASSES, CHUNKS)),
            dma((3,)), dma((3,)), dma((SLOTS, 2, 2)), dma((PIECES,)),
            dma((PASSES, PIECES)), dma((PASSES, PIECES)),
            dma((PASSES, PIECES)), dma((PASSES, PIECES)),
            dma((PASSES, SENT)), dma((PASSES, SENT)), dma((3,)), dma((3,)),
        ],
        compiler_params=pltpu.CompilerParams(
            collective_id=0, has_side_effects=True, vmem_limit_bytes=64 * 1024 * 1024 - 65536),
    )(
        expert_ids.T, gates.T, norm_gain[None, :], norm_bias[None, :],
        tokens, w_gate, w_up, w_down,
    )


def solution(mesh):
    groups_apart = EXPERTS == GROUP_EXPERTS * mesh.shape["ep"]
    fused = groups_apart and mesh.shape["ep"] == 4 and mesh.shape["tp"] == 4
    return jax.shard_map(
        fused_on_device if fused else on_device,
        mesh=mesh,
        in_specs=(
            P(("grp", "ep"), None),
            P(("grp", "ep"), None),
            P(("grp", "ep"), None),
            P("ep", None, "tp"),
            P("ep", None, "tp"),
            P("ep", "tp", None),
            P("tp"),
            P("tp"),
        ),
        out_specs=P(("grp", "ep"), "tp"),
        check_vma=False,
    )
```

```python
import functools
import jax
import jax.numpy as jnp
from jax import lax
from jax.experimental import pallas as pl
from jax.experimental.pallas import tpu as pltpu
from jax.sharding import PartitionSpec as P

D = 4096
TOPK = 2
EXPERTS = 16
CAP = 64


norm_eps = 1e-05


def route_slots(expert_ids):
    flat_ids = expert_ids.reshape(-1)
    onehot = (flat_ids[:, None] == jnp.arange(EXPERTS, dtype=jnp.int32)[None, :]).astype(jnp.int32)
    position = jnp.sum((jnp.cumsum(onehot, axis=0) - 1) * onehot, axis=1)
    target = flat_ids * CAP + position
    token_of = jnp.arange(flat_ids.shape[0], dtype=jnp.int32) // TOPK
    source = jnp.zeros((EXPERTS * CAP,), jnp.int32).at[target].set(token_of)
    filled = jnp.zeros((EXPERTS * CAP,), jnp.bool_).at[target].set(True)
    return (target, source, filled)


def on_device(tokens, expert_ids, gates, w_gate, w_up, w_down, norm_gain, norm_bias):
    tok_rows, width = tokens.shape
    piece_width = norm_gain.shape[0]
    target, source, filled = route_slots(expert_ids)
    outgoing = jnp.where(filled[:, None], tokens[source], jnp.zeros((), jnp.bfloat16)).reshape(
        EXPERTS, CAP, width
    )
    arrived = lax.all_to_all(outgoing, "ep", split_axis=0, concat_axis=1, tiled=True)
    gate_part = jnp.einsum("erd,edf->erf", arrived, w_gate, preferred_element_type=jnp.float32)
    up_part = jnp.einsum("erd,edf->erf", arrived, w_up, preferred_element_type=jnp.float32)
    hidden = (jax.nn.silu(gate_part) * up_part).astype(jnp.bfloat16)
    partial_value = jnp.einsum("erf,efd->erd", hidden, w_down, preferred_element_type=jnp.float32)
    summed = lax.psum_scatter(
        partial_value.astype(jnp.bfloat16), "tp", scatter_dimension=2, tiled=True
    )
    returned = lax.all_to_all(summed, "ep", split_axis=1, concat_axis=0, tiled=True)
    picked = returned.reshape(EXPERTS * CAP, piece_width)[target].reshape(
        tok_rows, TOPK, piece_width
    )
    combined = jnp.sum(picked.astype(jnp.float32) * gates[:, :, None], axis=1)
    stats = lax.psum((jnp.sum(combined, axis=1), jnp.sum(combined * combined, axis=1)), "tp")
    row_mean = stats[0] / D
    row_var = stats[1] / D - row_mean * row_mean
    normed = (combined - row_mean[:, None]) * lax.rsqrt(
        row_var[:, None] + norm_eps
    ) * norm_gain + norm_bias
    return normed.astype(jnp.bfloat16)


GROUP_EXPERTS = 4
CHUNKS = 16
HALF = CHUNKS // 2
PASSES = 2
SLOTS = 3
PIECES = 8
SENT = 6
HOP = 2
EARLY = 2
F32 = jnp.float32
BF16 = jnp.bfloat16
MESH = pl.DeviceIdType.MESH


def moe_kernel(
    ids_ref, gates_ref, gain_ref, bias_ref, tokens_ref, wg_ref, wu_ref, wd_ref,
    out_ref,
    tok, wbuf, wd, acc, hid, xr, dnb, place, collect, rowg, meta, meta_in,
    part, core_in, y_in, z_in, st_out, st_in,
    tok_sem, y_send, y_recv, z_send, z_recv, own_send, own_recv, fwd_send, fwd_recv,
    meta_send, meta_recv, w_sem, wd_sem, pc_send, pc_recv, py_send, py_recv,
    pz_send, pz_recv, st_send, st_recv,
):
    ep = lax.axis_index("ep")
    z = lax.axis_index("tp")
    y, c = ep // 2, ep % 2
    partner = y * 2 + (1 - c)
    across = (1 - y) * 2 + c
    diag = (1 - y) * 2 + (1 - c)
    par, side = z % 2, z // 2
    zpeer = z + 1 - 2 * par
    rows, width = tokens_ref.shape
    band = rows // PASSES
    experts = wg_ref.shape[0]
    cols = width // CHUNKS
    piece = gain_ref.shape[1]
    part_cols = piece // 2

    def remote(src, dst, send, recv, e, t):
        return pltpu.make_async_remote_copy(
            src_ref=src, dst_ref=dst, send_sem=send, recv_sem=recv,
            device_id={"ep": e, "tp": t}, device_id_type=MESH,
        )

    def span(ch, size):
        return pl.ds(pl.multiple_of(ch * size, size), size)

    def load_tok(ch):
        return pltpu.make_async_copy(
            tokens_ref.at[:, span(ch, cols)], tok.at[ch, ep], tok_sem.at[ch])

    def band_rows(h):
        return pl.ds(pl.multiple_of(h * band, band), band)

    def flip(far, near):
        return 2 * (side + far - 2 * side * far) + par + near - 2 * par * near

    def target(i):
        return flip((3 - i // 2) // 2, (3 - i // 2) % 2)

    def next_hop(i):
        return flip((i // 2) % 2, 1 - (i // 2) % 2)

    def load_wd(i):
        return pltpu.make_async_copy(
            wd_ref.at[:, :, span(target(i) * 2 + i % 2, part_cols)], wd.at[i], wd_sem.at[i])

    def direct(j):
        return par * HALF + j

    def swapped(j):
        return (1 - par) * HALF + j

    def unit_chunk(u):
        late, begun = u // 7, (u + 7) // 8
        kind = (1 - u % 2) * begun + late
        index = (u + 1) // 2 - (1 - u % 2) * begun - late
        return (par + kind - 2 * par * kind) * HALF + 2 * index

    def load_unit(t):
        first = unit_chunk(t % HALF)
        window = pl.ds(pl.multiple_of(first * cols, 2 * cols), 2 * cols)
        return [
            pltpu.make_async_copy(
                w_ref.at[:, window, :], wbuf.at[t % SLOTS, g], w_sem.at[t % SLOTS, g])
            for g, w_ref in enumerate((wg_ref, wu_ref))
        ]

    def y_copy(h, j):
        blk = tok.at[direct(j), ep, band_rows(h)]
        return remote(blk, blk, y_send.at[h, j], y_recv.at[h, j], across, z)

    def y_arrive(h, j):
        blk = tok.at[direct(j), across, band_rows(h)]
        return remote(blk, blk, y_send.at[h, j], y_recv.at[h, j], across, z)

    def z_copy(h, j):
        blk = tok.at[direct(j), across, band_rows(h)]
        return remote(blk, blk, z_send.at[h, j], z_recv.at[h, j], ep, zpeer)

    def z_arrive(h, j):
        blk = tok.at[swapped(j), across, band_rows(h)]
        return remote(blk, blk, z_send.at[h, j], z_recv.at[h, j], ep, zpeer)

    def own_copy(h, n):
        blk = tok.at[pl.ds(n * HALF, HALF), ep, band_rows(h)]
        return remote(blk, blk, own_send.at[h, n], own_recv.at[h, n], partner, z)

    def own_arrive(h, n):
        blk = tok.at[pl.ds(n * HALF, HALF), partner, band_rows(h)]
        return remote(blk, blk, own_send.at[h, n], own_recv.at[h, n], partner, z)

    def fwd_copy(h, ch):
        blk = tok.at[ch, across, band_rows(h)]
        return remote(blk, blk, fwd_send.at[h, ch], fwd_recv.at[h, ch], partner, z)

    def fwd_arrive(h, ch):
        blk = tok.at[ch, diag, band_rows(h)]
        return remote(blk, blk, fwd_send.at[h, ch], fwd_recv.at[h, ch], partner, z)

    def meta_copy(e, k):
        return remote(meta.at[e], meta_in.at[ep], meta_send.at[k], meta_recv.at[k], e, z)

    def meta_arrive(e, k):
        return remote(meta.at[e], meta_in.at[e], meta_send.at[k], meta_recv.at[k], e, z)

    peers = (partner, across, diag)

    for j in range(HALF):
        load_tok(direct(j)).start()
    for j in range(HALF):
        load_tok(swapped(j)).start()

    barrier = pltpu.get_barrier_semaphore()
    for e in peers:
        pl.semaphore_signal(barrier, inc=1, device_id={"ep": e, "tp": z}, device_id_type=MESH)
    for d in (1, 2, 3):
        pl.semaphore_signal(
            barrier, inc=1, device_id={"ep": ep, "tp": (z + d) % 4}, device_id_type=MESH)
    total_experts = 4 * experts
    expert_row = lax.broadcasted_iota(jnp.int32, (total_experts, rows), 0)
    first = ids_ref[0:1, :] == expert_row
    second = ids_ref[1:2, :] == expert_row
    named = jnp.where(first | second, 1.0, 0.0).astype(F32)
    weight = jnp.where(first, gates_ref[0:1, :], jnp.where(second, gates_ref[1:2, :], 0.0))
    tri_r = lax.broadcasted_iota(jnp.int32, (rows, rows), 0)
    tri_c = lax.broadcasted_iota(jnp.int32, (rows, rows), 1)
    before = jnp.where(
        (tri_r < tri_c) & (tri_r // band == tri_c // band), 1.0, 0.0).astype(BF16)
    position = jnp.dot(named.astype(BF16), before, preferred_element_type=F32)
    slot = jnp.where(
        named > 0.5, position + ((expert_row % experts) * CAP).astype(F32), -1.0)
    for e in range(4):
        meta[e, 0:experts, :] = slot[e * experts:(e + 1) * experts, :]
        meta[e, experts:2 * experts, :] = weight[e * experts:(e + 1) * experts, :]
    for ch in range(CHUNKS):
        load_tok(ch).wait()
    for t in range(SLOTS):
        for cp in load_unit(t):
            cp.start()
    for i in range(PIECES):
        load_wd(i).start()
    pl.semaphore_wait(barrier, 6)
    for k, e in enumerate(peers):
        meta_copy(e, k).start()
    for h in range(PASSES):
        for j in range(HALF):
            y_copy(h, j).start()
        for n in range(2):
            own_copy(h, n).start()

    meta_in[ep] = meta[ep]
    acc[...] = jnp.zeros_like(acc)
    for k, e in enumerate(peers):
        meta_arrive(e, k).wait_recv()
    for n in range(2):
        own_arrive(0, n).wait_recv()

    row_f = tri_r.astype(F32)
    for s in range(4):
        info = meta_in[s]
        put = jnp.zeros((rows, rows), F32)
        for e in range(experts):
            put += jnp.where(row_f == info[e:e + 1, :], 1.0, 0.0)
        back = put.T
        for h in range(PASSES):
            mine = slice(h * band, (h + 1) * band)
            place[h, s] = put[:, mine].astype(BF16)
            collect[h, s] = back[mine, :].astype(BF16)
            for e in range(experts):
                g = jnp.sum(
                    put[e * CAP:(e + 1) * CAP, mine]
                    * info[experts + e:experts + e + 1, mine],
                    axis=1, keepdims=True)
                rowg[h, e, s * CAP:(s + 1) * CAP, :] = jnp.broadcast_to(g, (CAP, 128))

    def unit(h, u):
        t = h * HALF + u
        chunks = [unit_chunk(u) + k for k in range(2)]
        for ch in chunks:
            fwd_arrive(h, ch).wait_recv()
        for cp in load_unit(t):
            cp.wait()
        for k, ch in enumerate(chunks):
            for s in range(4):
                x = jnp.dot(
                    place[h, s], tok[ch, s, band_rows(h), :],
                    preferred_element_type=F32).astype(BF16)
                for e in range(experts):
                    xr[e, s * CAP:(s + 1) * CAP, k * cols:(k + 1) * cols] = (
                        x[e * CAP:(e + 1) * CAP, :])
        for e in range(experts):
            for g in range(2):
                acc[g, e] += jnp.dot(xr[e], wbuf[t % SLOTS, g, e], preferred_element_type=F32)

        @pl.when(t + SLOTS < PASSES * HALF)
        def _():
            for cp in load_unit(t + SLOTS):
                cp.start()

    def relay(r):
        @pl.when(r < PASSES * HALF)
        def _():
            h, j = r // HALF, r % HALF
            y_arrive(h, j).wait_recv()
            z_copy(h, j).start()
            fwd_copy(h, direct(j)).start()

        @pl.when((r >= HOP) & (r < PASSES * HALF + HOP))
        def _():
            h, j = (r - HOP) // HALF, (r - HOP) % HALF
            z_arrive(h, j).wait_recv()
            fwd_copy(h, swapped(j)).start()

    def activate(h):
        def one(e, carry):
            g = acc[0, e]
            v = g / (1.0 + jnp.exp(-g)) * acc[1, e]
            hid[e] = (v * rowg[h, e][:, 0:1]).astype(BF16)
            if h + 1 < PASSES:
                acc[0, e] = jnp.zeros_like(g)
                acc[1, e] = jnp.zeros_like(g)
            return carry
        lax.fori_loop(0, experts, one, 0)

    def core_copy(h, i):
        return remote(
            part.at[i, 1 - c, :, band_rows(h)], core_in.at[i, :, band_rows(h)],
            pc_send.at[h, i], pc_recv.at[h, i], partner, z)

    def ret_copy(h, i):
        return remote(
            part.at[i, c, 1 - y, band_rows(h)], y_in.at[i, band_rows(h)],
            py_send.at[h, i], py_recv.at[h, i], across, z)

    def scatter_copy(h, i):
        return remote(
            part.at[i, c, y, band_rows(h)], z_in.at[i, band_rows(h)],
            pz_send.at[h, i], pz_recv.at[h, i], ep, next_hop(i))

    def down(h, i):
        if h == 0:
            load_wd(i).wait()

        for e in range(experts):
            o = jnp.dot(hid[e], wd[i, e], preferred_element_type=F32).astype(BF16)
            for s in range(4):
                dnb[s, e * CAP:(e + 1) * CAP, :] = o[s * CAP:(s + 1) * CAP, :]
        for s in range(4):
            part[i, s % 2, s // 2, band_rows(h), :] = jnp.dot(
                collect[h, s], dnb[s], preferred_element_type=F32).astype(BF16)
        core_copy(h, i).start()

    def give_back(h, i):
        core_copy(h, i).wait_recv()
        part[i, c, 1 - y, band_rows(h), :] += core_in[i, 1 - y, band_rows(h), :]
        ret_copy(h, i).start()

    def settle(h, k):
        ret_copy(h, k).wait_recv()
        part[k, c, y, band_rows(h), :] += (
            core_in[k, y, band_rows(h), :] + y_in[k, band_rows(h), :])

        @pl.when(k // 2 == 1)
        def _():
            scatter_copy(h, k - 2).wait_recv()
            part[k, c, y, band_rows(h), :] += z_in[k - 2, band_rows(h), :]

        @pl.when(k < SENT)
        def _():
            scatter_copy(h, k).start()

    for r in range(HOP):
        relay(r)

    def first_pass(u, carry):
        @pl.when((u >= 1) & (u <= 2))
        def _():
            relay(2 * u)
            relay(2 * u + 1)

        @pl.when(u >= 3)
        def _():
            relay(u + HOP + 1)
        unit(0, u)
        return carry
    lax.fori_loop(0, HALF, first_pass, 0)
    activate(0)
    for n in range(2):
        own_arrive(1, n).wait_recv()

    def second_pass(j, carry):
        down(0, j)
        for n in range(2):
            relay(HALF + HOP + 1 + 2 * j + n)
        unit(1, j)
        give_back(0, j)

        @pl.when(j >= EARLY)
        def _():
            settle(0, j - EARLY)
        return carry
    lax.fori_loop(0, HALF, second_pass, 0)
    activate(1)

    def last_down(i, carry):
        @pl.when(i < PIECES)
        def _():
            down(1, i)

        @pl.when(i >= 1)
        def _():
            give_back(1, i - 1)

        @pl.when((i % 2 == 1) & (i >= 3) & (i < 3 + 2 * EARLY))
        def _():
            settle(0, PIECES - EARLY + (i - 3) // 2)
        return carry
    lax.fori_loop(0, PIECES + 1, last_down, 0)

    def last_settle(k, carry):
        settle(1, k)
        return carry
    lax.fori_loop(0, PIECES, last_settle, 0)

    halves = []
    for n in range(2):
        half = part[SENT + n, c, y].astype(F32)
        for i in range(2 + n, SENT, 2):
            for h in range(PASSES):
                scatter_copy(h, i).wait_recv()
            half += z_in[i].astype(F32)
        halves.append(half)
    total = jnp.concatenate(halves, axis=1)

    local_mean = jnp.sum(total, axis=1, keepdims=True) * (1.0 / piece)
    gap = total - local_mean
    local_m2 = jnp.sum(gap * gap, axis=1, keepdims=True)
    mean_t = jnp.broadcast_to(local_mean, (rows, 128)).T
    m2_t = jnp.broadcast_to(local_m2, (rows, 128)).T
    st_out[0:8, :] = mean_t[0:8, :]
    st_out[8:16, :] = m2_t[0:8, :]

    def stat_copy(d):
        return remote(
            st_out, st_in.at[d - 1], st_send.at[d - 1], st_recv.at[d - 1], ep, (z + d) % 4)
    for d in (1, 2, 3):
        stat_copy(d).start()
    for d in (1, 2, 3):
        stat_copy(d).wait_recv()
    means = [st_out[0:8, :]] + [st_in[d, 0:8, :] for d in range(3)]
    m2s = [st_out[8:16, :]] + [st_in[d, 8:16, :] for d in range(3)]
    mean = (means[0] + means[1] + means[2] + means[3]) * 0.25
    m2 = m2s[0] + m2s[1] + m2s[2] + m2s[3]
    for m in means:
        m2 += (m - mean) * (m - mean) * piece
    scale = lax.rsqrt(m2 * (1.0 / width) + norm_eps)
    mean_col = jnp.broadcast_to(mean[0:1, :], (128, rows)).T[:, 0:1]
    scale_col = jnp.broadcast_to(scale[0:1, :], (128, rows)).T[:, 0:1]
    out_ref[...] = (
        (total - mean_col) * scale_col * gain_ref[...] + bias_ref[...]).astype(BF16)

    def sent_tokens(j, carry):
        for h in range(PASSES):
            y_copy(h, j).wait_send()
            z_copy(h, j).wait_send()
            for ch in (direct(j), swapped(j)):
                fwd_copy(h, ch).wait_send()
        return carry
    lax.fori_loop(0, HALF, sent_tokens, 0)
    for h in range(PASSES):
        for n in range(2):
            own_copy(h, n).wait_send()
    for k, e in enumerate(peers):
        meta_copy(e, k).wait_send()
    for h in range(PASSES):
        for i in range(PIECES):
            core_copy(h, i).wait_send()
            ret_copy(h, i).wait_send()
        for i in range(SENT):
            scatter_copy(h, i).wait_send()
    for d in (1, 2, 3):
        stat_copy(d).wait_send()


def fused_on_device(tokens, expert_ids, gates, w_gate, w_up, w_down, norm_gain, norm_bias):
    rows, width = tokens.shape
    experts, _, hidden = w_gate.shape
    piece = norm_gain.shape[0]
    cols = width // CHUNKS
    part_cols = piece // 2
    band = rows // PASSES
    dma = pltpu.SemaphoreType.DMA
    vmem = pl.BlockSpec(memory_space=pltpu.VMEM)
    hbm = pl.BlockSpec(memory_space=pl.ANY)
    return pl.pallas_call(
        moe_kernel,
        out_shape=jax.ShapeDtypeStruct((rows, piece), jnp.bfloat16),
        in_specs=[vmem] * 4 + [hbm] * 4,
        out_specs=vmem,
        scratch_shapes=[
            pltpu.VMEM((CHUNKS, 4, rows, cols), BF16),
            pltpu.VMEM((SLOTS, 2, experts, 2 * cols, hidden), BF16),
            pltpu.VMEM((PIECES, experts, hidden, part_cols), BF16),
            pltpu.VMEM((2, experts, 4 * CAP, hidden), F32),
            pltpu.VMEM((experts, 4 * CAP, hidden), BF16),
            pltpu.VMEM((experts, 4 * CAP, 2 * cols), BF16),
            pltpu.VMEM((4, experts * CAP, part_cols), BF16),
            pltpu.VMEM((PASSES, 4, experts * CAP, band), BF16),
            pltpu.VMEM((PASSES, 4, band, experts * CAP), BF16),
            pltpu.VMEM((PASSES, experts, 4 * CAP, 128), F32),
            pltpu.VMEM((4, 2 * experts, rows), F32),
            pltpu.VMEM((4, 2 * experts, rows), F32),
            pltpu.VMEM((PIECES, 2, 2, rows, part_cols), BF16),
            pltpu.VMEM((PIECES, 2, rows, part_cols), BF16),
            pltpu.VMEM((PIECES, rows, part_cols), BF16),
            pltpu.VMEM((SENT, rows, part_cols), BF16),
            pltpu.VMEM((16, rows), F32),
            pltpu.VMEM((3, 16, rows), F32),
            dma((CHUNKS,)), dma((PASSES, HALF)), dma((PASSES, HALF)),
            dma((PASSES, HALF)), dma((PASSES, HALF)),
            dma((PASSES, 2)), dma((PASSES, 2)), dma((PASSES, CHUNKS)), dma((PASSES, CHUNKS)),
            dma((3,)), dma((3,)), dma((SLOTS, 2)), dma((PIECES,)),
            dma((PASSES, PIECES)), dma((PASSES, PIECES)),
            dma((PASSES, PIECES)), dma((PASSES, PIECES)),
            dma((PASSES, SENT)), dma((PASSES, SENT)), dma((3,)), dma((3,)),
        ],
        compiler_params=pltpu.CompilerParams(
            collective_id=0, has_side_effects=True, vmem_limit_bytes=64 * 1024 * 1024 - 65536),
    )(
        expert_ids.T, gates.T, norm_gain[None, :], norm_bias[None, :],
        tokens, w_gate, w_up, w_down,
    )


def solution(mesh):
    groups_apart = EXPERTS == GROUP_EXPERTS * mesh.shape["ep"]
    fused = groups_apart and mesh.shape["ep"] == 4 and mesh.shape["tp"] == 4
    return jax.shard_map(
        fused_on_device if fused else on_device,
        mesh=mesh,
        in_specs=(
            P(("grp", "ep"), None),
            P(("grp", "ep"), None),
            P(("grp", "ep"), None),
            P("ep", None, "tp"),
            P("ep", None, "tp"),
            P("ep", "tp", None),
            P("tp"),
            P("tp"),
        ),
        out_specs=P(("grp", "ep"), "tp"),
        check_vma=False,
    )
```

```python
import functools
import jax
import jax.numpy as jnp
from jax import lax
from jax.experimental import pallas as pl
from jax.experimental.pallas import tpu as pltpu
from jax.sharding import PartitionSpec as P

D = 4096
TOPK = 2
EXPERTS = 16
CAP = 64


norm_eps = 1e-05


def route_slots(expert_ids):
    flat_ids = expert_ids.reshape(-1)
    onehot = (flat_ids[:, None] == jnp.arange(EXPERTS, dtype=jnp.int32)[None, :]).astype(jnp.int32)
    position = jnp.sum((jnp.cumsum(onehot, axis=0) - 1) * onehot, axis=1)
    target = flat_ids * CAP + position
    token_of = jnp.arange(flat_ids.shape[0], dtype=jnp.int32) // TOPK
    source = jnp.zeros((EXPERTS * CAP,), jnp.int32).at[target].set(token_of)
    filled = jnp.zeros((EXPERTS * CAP,), jnp.bool_).at[target].set(True)
    return (target, source, filled)


def on_device(tokens, expert_ids, gates, w_gate, w_up, w_down, norm_gain, norm_bias):
    tok_rows, width = tokens.shape
    piece_width = norm_gain.shape[0]
    target, source, filled = route_slots(expert_ids)
    outgoing = jnp.where(filled[:, None], tokens[source], jnp.zeros((), jnp.bfloat16)).reshape(
        EXPERTS, CAP, width
    )
    arrived = lax.all_to_all(outgoing, "ep", split_axis=0, concat_axis=1, tiled=True)
    gate_part = jnp.einsum("erd,edf->erf", arrived, w_gate, preferred_element_type=jnp.float32)
    up_part = jnp.einsum("erd,edf->erf", arrived, w_up, preferred_element_type=jnp.float32)
    hidden = (jax.nn.silu(gate_part) * up_part).astype(jnp.bfloat16)
    partial_value = jnp.einsum("erf,efd->erd", hidden, w_down, preferred_element_type=jnp.float32)
    summed = lax.psum_scatter(
        partial_value.astype(jnp.bfloat16), "tp", scatter_dimension=2, tiled=True
    )
    returned = lax.all_to_all(summed, "ep", split_axis=1, concat_axis=0, tiled=True)
    picked = returned.reshape(EXPERTS * CAP, piece_width)[target].reshape(
        tok_rows, TOPK, piece_width
    )
    combined = jnp.sum(picked.astype(jnp.float32) * gates[:, :, None], axis=1)
    stats = lax.psum((jnp.sum(combined, axis=1), jnp.sum(combined * combined, axis=1)), "tp")
    row_mean = stats[0] / D
    row_var = stats[1] / D - row_mean * row_mean
    normed = (combined - row_mean[:, None]) * lax.rsqrt(
        row_var[:, None] + norm_eps
    ) * norm_gain + norm_bias
    return normed.astype(jnp.bfloat16)


GROUP_EXPERTS = 4
CHUNKS = 16
HALF = CHUNKS // 2
PASSES = 2
SLOTS = 3
PIECES = 8
SENT = 6
FIRST_RELAYS = (
    ((0, 1), ()), ((2, 3), (0, 1)), ((4, 5), ()), ((6,), (2, 3)),
    ((7,), ()), ((8,), (4, 5)), ((9,), (6, 7)), ((10, 11, 12), (8,)),
)
SECOND_RELAYS = (
    ((13, 14, 15), (9, 10)), ((), (11,)), ((), (12, 13)), ((), (14, 15)),
    ((), ()), ((), ()), ((), ()), ((), ()),
)
SECOND_PIECES = (
    ((0, 1), (), ()), ((2,), (), ()), ((3,), (0,), (0,)), ((4,), (1,), (1,)),
    ((5,), (2,), ()), ((6,), (3,), (2,)), ((7,), (4,), (3,)), ((), (), (4,)),
)
LATE_SETTLES = ((4, 6), (6, 7))
LAST = 6
F32 = jnp.float32
BF16 = jnp.bfloat16
MESH = pl.DeviceIdType.MESH


def moe_kernel(
    ids_ref, gates_ref, gain_ref, bias_ref, tokens_ref, wg_ref, wu_ref, wd_ref,
    out_ref,
    tok, wbuf, wd, acc, hid, xr, dnb, place, collect, rowg, meta, meta_in,
    part, core_in, y_in, z_in, pair_in, st_out, st_in,
    tok_sem, y_send, y_recv, z_send, z_recv, own_send, own_recv, fwd_send, fwd_recv,
    meta_send, meta_recv, w_sem, wd_sem, pc_send, pc_recv, py_send, py_recv,
    pz_send, pz_recv, pair_send, pair_recv, st_send, st_recv,
):
    ep = lax.axis_index("ep")
    z = lax.axis_index("tp")
    y, c = ep // 2, ep % 2
    partner = y * 2 + (1 - c)
    across = (1 - y) * 2 + c
    diag = (1 - y) * 2 + (1 - c)
    par, side = z % 2, z // 2
    zpeer = z + 1 - 2 * par
    rows, width = tokens_ref.shape
    band = rows // PASSES
    experts = wg_ref.shape[0]
    cols = width // CHUNKS
    piece = gain_ref.shape[1]
    part_cols = piece // 2

    def remote(src, dst, send, recv, e, t):
        return pltpu.make_async_remote_copy(
            src_ref=src, dst_ref=dst, send_sem=send, recv_sem=recv,
            device_id={"ep": e, "tp": t}, device_id_type=MESH,
        )

    def span(ch, size):
        return pl.ds(pl.multiple_of(ch * size, size), size)

    def load_tok(ch):
        return pltpu.make_async_copy(
            tokens_ref.at[:, span(ch, cols)], tok.at[ch, ep], tok_sem.at[ch])

    def band_rows(h):
        return pl.ds(pl.multiple_of(h * band, band), band)

    inner = par + side - 2 * par * side
    paired = 5 - 4 * inner
    own = PIECES - 1

    def flip(far, near):
        return 2 * (side + far - 2 * side * far) + par + near - 2 * par * near

    def target(i):
        mask = (1 - inner) * (3 - i // 2) + inner * ((i // 2 + 1) % 4)
        return flip(mask // 2, mask % 2)

    def ranked(r):
        return r + (1 - inner) * (r // 5) + inner * ((r + 6) // 7)

    def load_wd(i):
        return pltpu.make_async_copy(
            wd_ref.at[:, :, span(target(i) * 2 + i % 2, part_cols)], wd.at[i], wd_sem.at[i])

    def direct(j):
        return par * HALF + j

    def swapped(j):
        return (1 - par) * HALF + j

    def unit_chunk(u):
        late, begun = u // 7, (u + 7) // 8
        kind = (1 - u % 2) * begun + late
        index = (u + 1) // 2 - (1 - u % 2) * begun - late
        return (par + kind - 2 * par * kind) * HALF + 2 * index

    def load_unit(t):
        first = unit_chunk(t % HALF)
        window = pl.ds(pl.multiple_of(first * cols, 2 * cols), 2 * cols)
        return [
            pltpu.make_async_copy(
                w_ref.at[:, window, :], wbuf.at[t % SLOTS, g], w_sem.at[t % SLOTS, g])
            for g, w_ref in enumerate((wg_ref, wu_ref))
        ]

    def y_copy(h, j):
        blk = tok.at[direct(j), ep, band_rows(h)]
        return remote(blk, blk, y_send.at[h, j], y_recv.at[h, j], across, z)

    def y_arrive(h, j):
        blk = tok.at[direct(j), across, band_rows(h)]
        return remote(blk, blk, y_send.at[h, j], y_recv.at[h, j], across, z)

    def z_copy(h, j):
        blk = tok.at[direct(j), across, band_rows(h)]
        return remote(blk, blk, z_send.at[h, j], z_recv.at[h, j], ep, zpeer)

    def z_arrive(h, j):
        blk = tok.at[swapped(j), across, band_rows(h)]
        return remote(blk, blk, z_send.at[h, j], z_recv.at[h, j], ep, zpeer)

    def own_copy(h, n):
        blk = tok.at[pl.ds(n * HALF, HALF), ep, band_rows(h)]
        return remote(blk, blk, own_send.at[h, n], own_recv.at[h, n], partner, z)

    def own_arrive(h, n):
        blk = tok.at[pl.ds(n * HALF, HALF), partner, band_rows(h)]
        return remote(blk, blk, own_send.at[h, n], own_recv.at[h, n], partner, z)

    def fwd_copy(h, ch):
        blk = tok.at[ch, across, band_rows(h)]
        return remote(blk, blk, fwd_send.at[h, ch], fwd_recv.at[h, ch], partner, z)

    def fwd_arrive(h, ch):
        blk = tok.at[ch, diag, band_rows(h)]
        return remote(blk, blk, fwd_send.at[h, ch], fwd_recv.at[h, ch], partner, z)

    def meta_copy(e, k):
        return remote(meta.at[e], meta_in.at[ep], meta_send.at[k], meta_recv.at[k], e, z)

    def meta_arrive(e, k):
        return remote(meta.at[e], meta_in.at[e], meta_send.at[k], meta_recv.at[k], e, z)

    peers = (partner, across, diag)

    for j in range(HALF):
        load_tok(direct(j)).start()
    for j in range(HALF):
        load_tok(swapped(j)).start()

    barrier = pltpu.get_barrier_semaphore()
    for e in peers:
        pl.semaphore_signal(barrier, inc=1, device_id={"ep": e, "tp": z}, device_id_type=MESH)
    for d in (1, 2, 3):
        pl.semaphore_signal(
            barrier, inc=1, device_id={"ep": ep, "tp": (z + d) % 4}, device_id_type=MESH)
    total_experts = 4 * experts
    expert_row = lax.broadcasted_iota(jnp.int32, (total_experts, rows), 0)
    first = ids_ref[0:1, :] == expert_row
    second = ids_ref[1:2, :] == expert_row
    named = jnp.where(first | second, 1.0, 0.0).astype(F32)
    weight = jnp.where(first, gates_ref[0:1, :], jnp.where(second, gates_ref[1:2, :], 0.0))
    tri_r = lax.broadcasted_iota(jnp.int32, (rows, rows), 0)
    tri_c = lax.broadcasted_iota(jnp.int32, (rows, rows), 1)
    before = jnp.where(
        (tri_r < tri_c) & (tri_r // band == tri_c // band), 1.0, 0.0).astype(BF16)
    position = jnp.dot(named.astype(BF16), before, preferred_element_type=F32)
    slot = jnp.where(
        named > 0.5, position + ((expert_row % experts) * CAP).astype(F32), -1.0)
    for e in range(4):
        meta[e, 0:experts, :] = slot[e * experts:(e + 1) * experts, :]
        meta[e, experts:2 * experts, :] = weight[e * experts:(e + 1) * experts, :]
    for ch in range(CHUNKS):
        load_tok(ch).wait()
    for t in range(SLOTS):
        for cp in load_unit(t):
            cp.start()
    for i in range(PIECES):
        load_wd(i).start()
    pl.semaphore_wait(barrier, 6)
    for k, e in enumerate(peers):
        meta_copy(e, k).start()
    for h in range(PASSES):
        for j in range(HALF):
            y_copy(h, j).start()
        for n in range(2):
            own_copy(h, n).start()

    meta_in[ep] = meta[ep]
    acc[...] = jnp.zeros_like(acc)
    for k, e in enumerate(peers):
        meta_arrive(e, k).wait_recv()
    for n in range(2):
        own_arrive(0, n).wait_recv()

    row_f = tri_r.astype(F32)
    for s in range(4):
        info = meta_in[s]
        put = jnp.zeros((rows, rows), F32)
        for e in range(experts):
            put += jnp.where(row_f == info[e:e + 1, :], 1.0, 0.0)
        back = put.T
        for h in range(PASSES):
            mine = slice(h * band, (h + 1) * band)
            place[h, s] = put[:, mine].astype(BF16)
            collect[h, s] = back[mine, :].astype(BF16)
            for e in range(experts):
                g = jnp.sum(
                    put[e * CAP:(e + 1) * CAP, mine]
                    * info[experts + e:experts + e + 1, mine],
                    axis=1, keepdims=True)
                rowg[h, e, s * CAP:(s + 1) * CAP, :] = jnp.broadcast_to(g, (CAP, 128))

    def unit(h, u):
        t = h * HALF + u
        chunks = [unit_chunk(u) + k for k in range(2)]
        for ch in chunks:
            fwd_arrive(h, ch).wait_recv()
        for cp in load_unit(t):
            cp.wait()
        for k, ch in enumerate(chunks):
            for s in range(4):
                x = jnp.dot(
                    place[h, s], tok[ch, s, band_rows(h), :],
                    preferred_element_type=F32).astype(BF16)
                for e in range(experts):
                    xr[e, s * CAP:(s + 1) * CAP, k * cols:(k + 1) * cols] = (
                        x[e * CAP:(e + 1) * CAP, :])
        for e in range(experts):
            for g in range(2):
                acc[g, e] += jnp.dot(xr[e], wbuf[t % SLOTS, g, e], preferred_element_type=F32)

        if t + SLOTS < PASSES * HALF:
            for cp in load_unit(t + SLOTS):
                cp.start()

    def relay_y(r):
        h, j = r // HALF, r % HALF
        y_arrive(h, j).wait_recv()
        z_copy(h, j).start()
        fwd_copy(h, direct(j)).start()

    def relay_z(r):
        h, j = r // HALF, r % HALF
        z_arrive(h, j).wait_recv()
        fwd_copy(h, swapped(j)).start()

    def relay(ys, zs):
        for r in ys:
            relay_y(r)
        for r in zs:
            relay_z(r)

    def activate(h):
        def one(e, carry):
            g = acc[0, e]
            v = g / (1.0 + jnp.exp(-g)) * acc[1, e]
            hid[e] = (v * rowg[h, e][:, 0:1]).astype(BF16)
            if h + 1 < PASSES:
                acc[0, e] = jnp.zeros_like(g)
                acc[1, e] = jnp.zeros_like(g)
            return carry
        lax.fori_loop(0, experts, one, 0)

    def core_copy(h, i):
        return remote(
            part.at[i, 1 - c, :, band_rows(h)], core_in.at[i, :, band_rows(h)],
            pc_send.at[h, i], pc_recv.at[h, i], partner, z)

    def ret_copy(h, i):
        return remote(
            part.at[i, c, 1 - y, band_rows(h)], y_in.at[i, band_rows(h)],
            py_send.at[h, i], py_recv.at[h, i], across, z)

    def scatter_slot(h, slot, i, dest):
        return remote(
            part.at[i, c, y, band_rows(h)], z_in.at[slot, band_rows(h)],
            pz_send.at[h, slot], pz_recv.at[h, slot], ep, dest)

    def scatter_copy(h, i):
        onward = inner * ((i + 6) // 8)
        return scatter_slot(
            h, i + 2 * inner * (i // 4), i, zpeer + onward * (target(i) - zpeer))

    def scattered(h, slot):
        return scatter_slot(h, slot, 0, zpeer)

    def down(h, i):
        if h == 0:
            load_wd(i).wait()

        for e in range(experts):
            o = jnp.dot(hid[e], wd[i, e], preferred_element_type=F32).astype(BF16)
            for s in range(4):
                dnb[s, e * CAP:(e + 1) * CAP, :] = o[s * CAP:(s + 1) * CAP, :]
        for s in range(4):
            part[i, s % 2, s // 2, band_rows(h), :] = jnp.dot(
                collect[h, s], dnb[s], preferred_element_type=F32).astype(BF16)
        core_copy(h, i).start()

    def pair_copy(n):
        return remote(
            part.at[paired, c, (1 - y) + n * (2 * y - 1), band_rows(1)], pair_in.at[n],
            pair_send.at[n], pair_recv.at[n], ep, zpeer)

    def give_pair():
        core_copy(1, paired).wait_recv()
        part[paired, c, :, band_rows(1), :] += core_in[paired, :, band_rows(1), :]
        for n in range(2):
            pair_copy(n).start()

    def give_own():
        core_copy(1, own).wait_recv()
        pair_copy(0).wait_recv()
        part[own, c, 1 - y, band_rows(1), :] += (
            core_in[own, 1 - y, band_rows(1), :] + pair_in[0])
        ret_copy(1, own).start()

    def give_back(h, i):
        core_copy(h, i).wait_recv()
        part[i, c, 1 - y, band_rows(h), :] += core_in[i, 1 - y, band_rows(h), :]
        ret_copy(h, i).start()

    def settle(h, i):
        ret_copy(h, i).wait_recv()
        part[i, c, y, band_rows(h), :] += (
            core_in[i, y, band_rows(h), :] + y_in[i, band_rows(h), :])

        @pl.when((inner == 1) & (i >= 2) & (i < SENT))
        def _():
            scattered(h, i - 2).wait_recv()
            part[i, c, y, band_rows(h), :] += z_in[i - 2, band_rows(h), :]

        @pl.when(i < SENT)
        def _():
            scatter_copy(h, i).start()

    for u in range(HALF):
        relay(*FIRST_RELAYS[u])
        unit(0, u)
    activate(0)
    for n in range(2):
        own_arrive(1, n).wait_recv()

    for u in range(HALF):
        downs, outer_settles, inner_settles = SECOND_PIECES[u]
        for i in downs:
            down(0, i)
        if u == 0:
            give_back(0, 0)
        relay(*SECOND_RELAYS[u])
        unit(1, u)
        for i in downs:
            if i != 0:
                give_back(0, i)
        for v, settles in enumerate((outer_settles, inner_settles)):
            for i in settles:
                @pl.when(inner == v)
                def _():
                    settle(0, i)
    activate(1)
    settle(0, SENT - 1)

    def nth(n):
        second = (8 - n) // 7 - (7 - n) // 7
        r = n - (n + 6) // 8
        return second * paired + (1 - second) * ranked(r)

    def last_down(n, carry):
        @pl.when(n < PIECES)
        def _():
            down(1, nth(n))

        @pl.when(n == 2)
        def _():
            give_pair()

        @pl.when((n >= 1) & (n != 2))
        def _():
            give_back(1, nth(n - 1))
        for step, i in LATE_SETTLES:
            @pl.when(n == step)
            def _():
                settle(0, i)

        @pl.when(n == 6 + inner)
        def _():
            settle(1, ranked(0))
        return carry
    lax.fori_loop(0, PIECES, last_down, 0)

    def stat_copy(h, d):
        return remote(
            st_out.at[h], st_in.at[h, d - 1],
            st_send.at[h, d - 1], st_recv.at[h, d - 1], ep, (z + d) % 4)

    def collect_total(h):
        for n in range(2):
            half = part[SENT + n, c, y, band_rows(h), :].astype(F32)
            for k in (n, 2 + n) if h == 0 or n == 0 else (2 + n,):
                slot = 4 * inner + k
                scattered(h, slot).wait_recv()
                half += z_in[slot, band_rows(h), :].astype(F32)
            acc[0, n, h * band:(h + 1) * band, :] = half

    def send_stats(h):
        mine = slice(h * band, (h + 1) * band)
        total = jnp.concatenate([acc[0, n, mine, :] for n in range(2)], axis=1)
        local_mean = jnp.sum(total, axis=1, keepdims=True) * (1.0 / piece)
        gap = total - local_mean
        local_m2 = jnp.sum(gap * gap, axis=1, keepdims=True)
        st_out[h, 0:8, :] = jnp.broadcast_to(local_mean, (band, 128)).T[0:8, :]
        st_out[h, 8:16, :] = jnp.broadcast_to(local_m2, (band, 128)).T[0:8, :]
        for d in (1, 2, 3):
            stat_copy(h, d).start()

    def normalize(h):
        mine = slice(h * band, (h + 1) * band)
        for d in (1, 2, 3):
            stat_copy(h, d).wait_recv()
        means = [st_out[h, 0:8, :]] + [st_in[h, d, 0:8, :] for d in range(3)]
        m2s = [st_out[h, 8:16, :]] + [st_in[h, d, 8:16, :] for d in range(3)]
        mean = (means[0] + means[1] + means[2] + means[3]) * 0.25
        m2 = m2s[0] + m2s[1] + m2s[2] + m2s[3]
        for m in means:
            m2 += (m - mean) * (m - mean) * piece
        scale = lax.rsqrt(m2 * (1.0 / width) + norm_eps)
        mean_col = jnp.broadcast_to(mean[0:1, :], (128, band)).T[:, 0:1]
        scale_col = jnp.broadcast_to(scale[0:1, :], (128, band)).T[:, 0:1]
        for n in range(2):
            cut = slice(n * part_cols, (n + 1) * part_cols)
            out_ref[mine, cut] = (
                (acc[0, n, mine, :] - mean_col) * scale_col * gain_ref[:, cut]
                + bias_ref[:, cut]).astype(BF16)

    def last_settle(r, carry):
        settle(1, ranked(r))
        return carry
    lax.fori_loop(1, 2, last_settle, 0)
    collect_total(0)
    send_stats(0)
    give_own()
    lax.fori_loop(2, LAST - 1, last_settle, 0)
    settle(1, ranked(LAST - 1))
    ret_copy(1, own).wait_recv()
    pair_copy(1).wait_recv()
    part[own, c, y, band_rows(1), :] += (
        core_in[own, y, band_rows(1), :] + y_in[own, band_rows(1), :] + pair_in[1])
    collect_total(1)
    send_stats(1)
    normalize(0)
    normalize(1)

    def sent_tokens(j, carry):
        for h in range(PASSES):
            y_copy(h, j).wait_send()
            z_copy(h, j).wait_send()
            for ch in (direct(j), swapped(j)):
                fwd_copy(h, ch).wait_send()
        return carry
    lax.fori_loop(0, HALF, sent_tokens, 0)
    for h in range(PASSES):
        for n in range(2):
            own_copy(h, n).wait_send()
    for k, e in enumerate(peers):
        meta_copy(e, k).wait_send()
    for n in range(2):
        pair_copy(n).wait_send()
    for h in range(PASSES):
        for i in range(PIECES):
            core_copy(h, i).wait_send()
        for d in (1, 2, 3):
            stat_copy(h, d).wait_send()
    for i in range(PIECES):
        ret_copy(0, i).wait_send()
        if i < SENT:
            scatter_copy(0, i).wait_send()
    for r in range(LAST + 1):
        ret_copy(1, ranked(r)).wait_send()
        if r < LAST - 1:
            scatter_copy(1, ranked(r)).wait_send()


def fused_on_device(tokens, expert_ids, gates, w_gate, w_up, w_down, norm_gain, norm_bias):
    rows, width = tokens.shape
    experts, _, hidden = w_gate.shape
    piece = norm_gain.shape[0]
    cols = width // CHUNKS
    part_cols = piece // 2
    band = rows // PASSES
    dma = pltpu.SemaphoreType.DMA
    vmem = pl.BlockSpec(memory_space=pltpu.VMEM)
    hbm = pl.BlockSpec(memory_space=pl.ANY)
    return pl.pallas_call(
        moe_kernel,
        out_shape=jax.ShapeDtypeStruct((rows, piece), jnp.bfloat16),
        in_specs=[vmem] * 4 + [hbm] * 4,
        out_specs=vmem,
        scratch_shapes=[
            pltpu.VMEM((CHUNKS, 4, rows, cols), BF16),
            pltpu.VMEM((SLOTS, 2, experts, 2 * cols, hidden), BF16),
            pltpu.VMEM((PIECES, experts, hidden, part_cols), BF16),
            pltpu.VMEM((2, experts, 4 * CAP, hidden), F32),
            pltpu.VMEM((experts, 4 * CAP, hidden), BF16),
            pltpu.VMEM((experts, 4 * CAP, 2 * cols), BF16),
            pltpu.VMEM((4, experts * CAP, part_cols), BF16),
            pltpu.VMEM((PASSES, 4, experts * CAP, band), BF16),
            pltpu.VMEM((PASSES, 4, band, experts * CAP), BF16),
            pltpu.VMEM((PASSES, experts, 4 * CAP, 128), F32),
            pltpu.VMEM((4, 2 * experts, rows), F32),
            pltpu.VMEM((4, 2 * experts, rows), F32),
            pltpu.VMEM((PIECES, 2, 2, rows, part_cols), BF16),
            pltpu.VMEM((PIECES, 2, rows, part_cols), BF16),
            pltpu.VMEM((PIECES, rows, part_cols), BF16),
            pltpu.VMEM((PIECES, rows, part_cols), BF16),
            pltpu.VMEM((2, band, part_cols), BF16),
            pltpu.VMEM((PASSES, 16, band), F32),
            pltpu.VMEM((PASSES, 3, 16, band), F32),
            dma((CHUNKS,)), dma((PASSES, HALF)), dma((PASSES, HALF)),
            dma((PASSES, HALF)), dma((PASSES, HALF)),
            dma((PASSES, 2)), dma((PASSES, 2)), dma((PASSES, CHUNKS)), dma((PASSES, CHUNKS)),
            dma((3,)), dma((3,)), dma((SLOTS, 2)), dma((PIECES,)),
            dma((PASSES, PIECES)), dma((PASSES, PIECES)),
            dma((PASSES, PIECES)), dma((PASSES, PIECES)),
            dma((PASSES, PIECES)), dma((PASSES, PIECES)), dma((2,)), dma((2,)),
            dma((PASSES, 3)), dma((PASSES, 3)),
        ],
        compiler_params=pltpu.CompilerParams(
            collective_id=0, has_side_effects=True, vmem_limit_bytes=64 * 1024 * 1024 - 65536),
    )(
        expert_ids.T, gates.T, norm_gain[None, :], norm_bias[None, :],
        tokens, w_gate, w_up, w_down,
    )


def solution(mesh):
    groups_apart = EXPERTS == GROUP_EXPERTS * mesh.shape["ep"]
    fused = groups_apart and mesh.shape["ep"] == 4 and mesh.shape["tp"] == 4
    return jax.shard_map(
        fused_on_device if fused else on_device,
        mesh=mesh,
        in_specs=(
            P(("grp", "ep"), None),
            P(("grp", "ep"), None),
            P(("grp", "ep"), None),
            P("ep", None, "tp"),
            P("ep", None, "tp"),
            P("ep", "tp", None),
            P("tp"),
            P("tp"),
        ),
        out_specs=P(("grp", "ep"), "tp"),
        check_vma=False,
    )
```

```python
import functools
import jax
import jax.numpy as jnp
from jax import lax
from jax.experimental import pallas as pl
from jax.experimental.pallas import tpu as pltpu
from jax.sharding import PartitionSpec as P

D = 4096
TOPK = 2
EXPERTS = 16
CAP = 64


norm_eps = 1e-05


def route_slots(expert_ids):
    flat_ids = expert_ids.reshape(-1)
    onehot = (flat_ids[:, None] == jnp.arange(EXPERTS, dtype=jnp.int32)[None, :]).astype(jnp.int32)
    position = jnp.sum((jnp.cumsum(onehot, axis=0) - 1) * onehot, axis=1)
    target = flat_ids * CAP + position
    token_of = jnp.arange(flat_ids.shape[0], dtype=jnp.int32) // TOPK
    source = jnp.zeros((EXPERTS * CAP,), jnp.int32).at[target].set(token_of)
    filled = jnp.zeros((EXPERTS * CAP,), jnp.bool_).at[target].set(True)
    return (target, source, filled)


def on_device(tokens, expert_ids, gates, w_gate, w_up, w_down, norm_gain, norm_bias):
    tok_rows, width = tokens.shape
    piece_width = norm_gain.shape[0]
    target, source, filled = route_slots(expert_ids)
    outgoing = jnp.where(filled[:, None], tokens[source], jnp.zeros((), jnp.bfloat16)).reshape(
        EXPERTS, CAP, width
    )
    arrived = lax.all_to_all(outgoing, "ep", split_axis=0, concat_axis=1, tiled=True)
    gate_part = jnp.einsum("erd,edf->erf", arrived, w_gate, preferred_element_type=jnp.float32)
    up_part = jnp.einsum("erd,edf->erf", arrived, w_up, preferred_element_type=jnp.float32)
    hidden = (jax.nn.silu(gate_part) * up_part).astype(jnp.bfloat16)
    partial_value = jnp.einsum("erf,efd->erd", hidden, w_down, preferred_element_type=jnp.float32)
    summed = lax.psum_scatter(
        partial_value.astype(jnp.bfloat16), "tp", scatter_dimension=2, tiled=True
    )
    returned = lax.all_to_all(summed, "ep", split_axis=1, concat_axis=0, tiled=True)
    picked = returned.reshape(EXPERTS * CAP, piece_width)[target].reshape(
        tok_rows, TOPK, piece_width
    )
    combined = jnp.sum(picked.astype(jnp.float32) * gates[:, :, None], axis=1)
    stats = lax.psum((jnp.sum(combined, axis=1), jnp.sum(combined * combined, axis=1)), "tp")
    row_mean = stats[0] / D
    row_var = stats[1] / D - row_mean * row_mean
    normed = (combined - row_mean[:, None]) * lax.rsqrt(
        row_var[:, None] + norm_eps
    ) * norm_gain + norm_bias
    return normed.astype(jnp.bfloat16)


GROUP_EXPERTS = 4
CHUNKS = 16
HALF = CHUNKS // 2
PASSES = 2
SLOTS = 3
PIECES = 8
SENT = 6
FIRST_RELAYS = (
    ((0, 1), ()), ((2, 3), (0, 1)), ((4, 5), ()), ((6,), (2, 3)),
    ((7,), ()), ((8,), (4, 5)), ((9,), (6, 7)), ((10, 11, 12), (8,)),
)
SECOND_RELAYS = (
    ((13, 14, 15), (9, 10)), ((), (11,)), ((), (12, 13)), ((), (14, 15)),
    ((), ()), ((), ()), ((), ()), ((), ()),
)
SECOND_PIECES = (
    ((0, 1), (), ()), ((2,), (), ()), ((3,), (0,), (0,)), ((4,), (1,), (1,)),
    ((5,), (2,), ()), ((6,), (3,), (2,)), ((7,), (4,), (3,)), ((), (), (4,)),
)
LATE_SETTLES = ((4, 6), (6, 7))
LAST = 6
F32 = jnp.float32
BF16 = jnp.bfloat16
MESH = pl.DeviceIdType.MESH


def moe_kernel(
    ids_ref, gates_ref, gain_ref, bias_ref, tokens_ref, wg_ref, wu_ref, wd_ref,
    out_ref,
    tok, wbuf, wd, acc, hid, xr, dnb, place, collect, rowg, meta, meta_in,
    part, core_in, y_in, z_in, pair_in, st_out, st_in,
    tok_sem, y_send, y_recv, z_send, z_recv, own_send, own_recv, fwd_send, fwd_recv,
    meta_send, meta_recv, w_sem, wd_sem, pc_send, pc_recv, py_send, py_recv,
    pz_send, pz_recv, pair_send, pair_recv, st_send, st_recv,
):
    ep = lax.axis_index("ep")
    z = lax.axis_index("tp")
    y, c = ep // 2, ep % 2
    partner = y * 2 + (1 - c)
    across = (1 - y) * 2 + c
    diag = (1 - y) * 2 + (1 - c)
    par, side = z % 2, z // 2
    zpeer = z + 1 - 2 * par
    rows, width = tokens_ref.shape
    band = rows // PASSES
    experts = wg_ref.shape[0]
    cols = width // CHUNKS
    piece = gain_ref.shape[1]
    part_cols = piece // 2

    def remote(src, dst, send, recv, e, t):
        return pltpu.make_async_remote_copy(
            src_ref=src, dst_ref=dst, send_sem=send, recv_sem=recv,
            device_id={"ep": e, "tp": t}, device_id_type=MESH,
        )

    def span(ch, size):
        return pl.ds(pl.multiple_of(ch * size, size), size)

    def load_tok(ch):
        return pltpu.make_async_copy(
            tokens_ref.at[:, span(ch, cols)], tok.at[ch, ep], tok_sem.at[ch])

    def band_rows(h):
        return pl.ds(pl.multiple_of(h * band, band), band)

    inner = par + side - 2 * par * side
    paired = 5 - 4 * inner
    own = PIECES - 1

    def flip(far, near):
        return 2 * (side + far - 2 * side * far) + par + near - 2 * par * near

    def target(i):
        mask = (1 - inner) * (3 - i // 2) + inner * ((i // 2 + 1) % 4)
        return flip(mask // 2, mask % 2)

    def ranked(r):
        return r + (1 - inner) * (r // 5) + inner * ((r + 6) // 7)

    def load_wd(i):
        return pltpu.make_async_copy(
            wd_ref.at[:, :, span(target(i) * 2 + i % 2, part_cols)], wd.at[i], wd_sem.at[i])

    def direct(j):
        return par * HALF + j

    def swapped(j):
        return (1 - par) * HALF + j

    def unit_chunk(u):
        late, begun = u // 7, (u + 7) // 8
        kind = (1 - u % 2) * begun + late
        index = (u + 1) // 2 - (1 - u % 2) * begun - late
        return (par + kind - 2 * par * kind) * HALF + 2 * index

    def load_unit(t):
        first = unit_chunk(t % HALF)
        window = pl.ds(pl.multiple_of(first * cols, 2 * cols), 2 * cols)
        return [
            pltpu.make_async_copy(
                w_ref.at[:, window, :], wbuf.at[t % SLOTS, g], w_sem.at[t % SLOTS, g])
            for g, w_ref in enumerate((wg_ref, wu_ref))
        ]

    def y_copy(h, j):
        blk = tok.at[direct(j), ep, band_rows(h)]
        return remote(blk, blk, y_send.at[h, j], y_recv.at[h, j], across, z)

    def y_arrive(h, j):
        blk = tok.at[direct(j), across, band_rows(h)]
        return remote(blk, blk, y_send.at[h, j], y_recv.at[h, j], across, z)

    def z_copy(h, j):
        blk = tok.at[direct(j), across, band_rows(h)]
        return remote(blk, blk, z_send.at[h, j], z_recv.at[h, j], ep, zpeer)

    def z_arrive(h, j):
        blk = tok.at[swapped(j), across, band_rows(h)]
        return remote(blk, blk, z_send.at[h, j], z_recv.at[h, j], ep, zpeer)

    def own_copy(h, n):
        blk = tok.at[pl.ds(n * HALF, HALF), ep, band_rows(h)]
        return remote(blk, blk, own_send.at[h, n], own_recv.at[h, n], partner, z)

    def own_arrive(h, n):
        blk = tok.at[pl.ds(n * HALF, HALF), partner, band_rows(h)]
        return remote(blk, blk, own_send.at[h, n], own_recv.at[h, n], partner, z)

    def fwd_copy(h, ch):
        blk = tok.at[ch, across, band_rows(h)]
        return remote(blk, blk, fwd_send.at[h, ch], fwd_recv.at[h, ch], partner, z)

    def fwd_arrive(h, ch):
        blk = tok.at[ch, diag, band_rows(h)]
        return remote(blk, blk, fwd_send.at[h, ch], fwd_recv.at[h, ch], partner, z)

    def meta_copy(e, k):
        return remote(meta.at[e], meta_in.at[ep], meta_send.at[k], meta_recv.at[k], e, z)

    def meta_arrive(e, k):
        return remote(meta.at[e], meta_in.at[e], meta_send.at[k], meta_recv.at[k], e, z)

    peers = (partner, across, diag)

    for j in range(HALF):
        load_tok(direct(j)).start()
    for j in range(HALF):
        load_tok(swapped(j)).start()

    barrier = pltpu.get_barrier_semaphore()
    for e in peers:
        pl.semaphore_signal(barrier, inc=1, device_id={"ep": e, "tp": z}, device_id_type=MESH)
    for d in (1, 2, 3):
        pl.semaphore_signal(
            barrier, inc=1, device_id={"ep": ep, "tp": (z + d) % 4}, device_id_type=MESH)
    total_experts = 4 * experts
    expert_row = lax.broadcasted_iota(jnp.int32, (total_experts, rows), 0)
    first = ids_ref[0:1, :] == expert_row
    second = ids_ref[1:2, :] == expert_row
    named = jnp.where(first | second, 1.0, 0.0).astype(F32)
    weight = jnp.where(first, gates_ref[0:1, :], jnp.where(second, gates_ref[1:2, :], 0.0))
    tri_r = lax.broadcasted_iota(jnp.int32, (rows, rows), 0)
    tri_c = lax.broadcasted_iota(jnp.int32, (rows, rows), 1)
    before = jnp.where(
        (tri_r < tri_c) & (tri_r // band == tri_c // band), 1.0, 0.0).astype(BF16)
    position = jnp.dot(named.astype(BF16), before, preferred_element_type=F32)
    slot = jnp.where(
        named > 0.5, position + ((expert_row % experts) * CAP).astype(F32), -1.0)
    for e in range(4):
        meta[e, 0:experts, :] = slot[e * experts:(e + 1) * experts, :]
        meta[e, experts:2 * experts, :] = weight[e * experts:(e + 1) * experts, :]
    for ch in range(CHUNKS):
        load_tok(ch).wait()
    for t in range(SLOTS):
        for cp in load_unit(t):
            cp.start()
    for i in range(PIECES):
        load_wd(i).start()
    pl.semaphore_wait(barrier, 6)
    for k, e in enumerate(peers):
        meta_copy(e, k).start()
    for h in range(PASSES):
        for j in range(HALF):
            y_copy(h, j).start()
        for n in range(2):
            own_copy(h, n).start()

    meta_in[ep] = meta[ep]
    acc[...] = jnp.zeros_like(acc)
    for k, e in enumerate(peers):
        meta_arrive(e, k).wait_recv()
    for n in range(2):
        own_arrive(0, n).wait_recv()

    row_f = tri_r.astype(F32)
    for s in range(4):
        info = meta_in[s]
        put = jnp.zeros((rows, rows), F32)
        for e in range(experts):
            put += jnp.where(row_f == info[e:e + 1, :], 1.0, 0.0)
        back = put.T
        for h in range(PASSES):
            mine = slice(h * band, (h + 1) * band)
            place[h, s] = put[:, mine].astype(BF16)
            collect[h, s] = back[mine, :].astype(BF16)
            for e in range(experts):
                g = jnp.sum(
                    put[e * CAP:(e + 1) * CAP, mine]
                    * info[experts + e:experts + e + 1, mine],
                    axis=1, keepdims=True)
                rowg[h, e, s * CAP:(s + 1) * CAP, :] = jnp.broadcast_to(g, (CAP, 128))

    def unit(h, u):
        t = h * HALF + u
        chunks = [unit_chunk(u) + k for k in range(2)]
        for ch in chunks:
            fwd_arrive(h, ch).wait_recv()
        for cp in load_unit(t):
            cp.wait()
        for k, ch in enumerate(chunks):
            for s in range(4):
                x = jnp.dot(
                    place[h, s], tok[ch, s, band_rows(h), :],
                    preferred_element_type=F32).astype(BF16)
                for e in range(experts):
                    xr[e, s * CAP:(s + 1) * CAP, k * cols:(k + 1) * cols] = (
                        x[e * CAP:(e + 1) * CAP, :])
        for e in range(experts):
            for g in range(2):
                acc[g, e] += jnp.dot(xr[e], wbuf[t % SLOTS, g, e], preferred_element_type=F32)

        if t + SLOTS < PASSES * HALF:
            for cp in load_unit(t + SLOTS):
                cp.start()

    def relay_y(r):
        h, j = r // HALF, r % HALF
        y_arrive(h, j).wait_recv()
        z_copy(h, j).start()
        fwd_copy(h, direct(j)).start()

    def relay_z(r):
        h, j = r // HALF, r % HALF
        z_arrive(h, j).wait_recv()
        fwd_copy(h, swapped(j)).start()

    def relay(ys, zs):
        for r in ys:
            relay_y(r)
        for r in zs:
            relay_z(r)

    def activate(h):
        def one(e, carry):
            g = acc[0, e]
            v = g / (1.0 + jnp.exp(-g)) * acc[1, e]
            hid[e] = (v * rowg[h, e][:, 0:1]).astype(BF16)
            if h + 1 < PASSES:
                acc[0, e] = jnp.zeros_like(g)
                acc[1, e] = jnp.zeros_like(g)
            return carry
        lax.fori_loop(0, experts, one, 0)

    def core_copy(h, i):
        return remote(
            part.at[i, 1 - c, :, band_rows(h)], core_in.at[i, :, band_rows(h)],
            pc_send.at[h, i], pc_recv.at[h, i], partner, z)

    def ret_copy(h, i):
        return remote(
            part.at[i, c, 1 - y, band_rows(h)], y_in.at[i, band_rows(h)],
            py_send.at[h, i], py_recv.at[h, i], across, z)

    def scatter_slot(h, slot, i, dest):
        return remote(
            part.at[i, c, y, band_rows(h)], z_in.at[slot, band_rows(h)],
            pz_send.at[h, slot], pz_recv.at[h, slot], ep, dest)

    def scatter_copy(h, i):
        onward = inner * ((i + 6) // 8)
        return scatter_slot(
            h, i + 2 * inner * (i // 4), i, zpeer + onward * (target(i) - zpeer))

    def scattered(h, slot):
        return scatter_slot(h, slot, 0, zpeer)

    def down(h, i):
        if h == 0:
            load_wd(i).wait()

        for e in range(experts):
            o = jnp.dot(hid[e], wd[i, e], preferred_element_type=F32).astype(BF16)
            for s in range(4):
                dnb[s, e * CAP:(e + 1) * CAP, :] = o[s * CAP:(s + 1) * CAP, :]
        for s in range(4):
            part[i, s % 2, s // 2, band_rows(h), :] = jnp.dot(
                collect[h, s], dnb[s], preferred_element_type=F32).astype(BF16)
        core_copy(h, i).start()

    def pair_copy(n):
        return remote(
            part.at[paired, c, (1 - y) + n * (2 * y - 1), band_rows(1)], pair_in.at[n],
            pair_send.at[n], pair_recv.at[n], ep, zpeer)

    def give_pair():
        core_copy(1, paired).wait_recv()
        part[paired, c, :, band_rows(1), :] += core_in[paired, :, band_rows(1), :]
        pair_copy(0).start()

        @pl.when(inner == 1)
        def _():
            pair_copy(1).start()

    def give_own():
        core_copy(1, own).wait_recv()
        pair_copy(0).wait_recv()
        part[own, c, 1 - y, band_rows(1), :] += (
            core_in[own, 1 - y, band_rows(1), :] + pair_in[0])
        ret_copy(1, own).start()

    def give_back(h, i):
        core_copy(h, i).wait_recv()
        part[i, c, 1 - y, band_rows(h), :] += core_in[i, 1 - y, band_rows(h), :]
        ret_copy(h, i).start()

    def settle(h, i):
        ret_copy(h, i).wait_recv()
        part[i, c, y, band_rows(h), :] += (
            core_in[i, y, band_rows(h), :] + y_in[i, band_rows(h), :])

        @pl.when((inner == 1) & (i >= 2) & (i < SENT))
        def _():
            scattered(h, i - 2).wait_recv()
            part[i, c, y, band_rows(h), :] += z_in[i - 2, band_rows(h), :]

        @pl.when(i < SENT)
        def _():
            scatter_copy(h, i).start()

    for u in range(HALF):
        relay(*FIRST_RELAYS[u])
        unit(0, u)
    activate(0)
    for n in range(2):
        own_arrive(1, n).wait_recv()

    for u in range(HALF):
        downs, outer_settles, inner_settles = SECOND_PIECES[u]
        for i in downs:
            down(0, i)
        if u == 0:
            give_back(0, 0)
        relay(*SECOND_RELAYS[u])
        unit(1, u)
        for i in downs:
            if i != 0:
                give_back(0, i)
        for v, settles in enumerate((outer_settles, inner_settles)):
            for i in settles:
                @pl.when(inner == v)
                def _():
                    settle(0, i)
    activate(1)

    def nth(n):
        second = (8 - n) // 7 - (7 - n) // 7
        r = n - (n + 6) // 8
        return second * paired + (1 - second) * ranked(r)

    def last_down(n, carry):
        @pl.when(n < PIECES)
        def _():
            down(1, nth(n))

        @pl.when(n == 2)
        def _():
            give_pair()

        @pl.when((n >= 1) & (n != 2))
        def _():
            give_back(1, nth(n - 1))
        for step, i in LATE_SETTLES:
            @pl.when(n == step)
            def _():
                settle(0, i)

        @pl.when(n == inner)
        def _():
            settle(0, SENT - 1)

        @pl.when(n == 6 + inner)
        def _():
            settle(1, ranked(0))
        return carry
    lax.fori_loop(0, PIECES, last_down, 0)

    def stat_copy(h, d):
        return remote(
            st_out.at[h], st_in.at[h, d - 1],
            st_send.at[h, d - 1], st_recv.at[h, d - 1], ep, (z + d) % 4)

    def collect_total(h):
        for n in range(2):
            half = part[SENT + n, c, y, band_rows(h), :].astype(F32)
            for k in (n, 2 + n) if h == 0 or n == 0 else (2 + n,):
                slot = 4 * inner + k
                scattered(h, slot).wait_recv()
                half += z_in[slot, band_rows(h), :].astype(F32)
            acc[0, n, h * band:(h + 1) * band, :] = half

    def send_stats(h):
        mine = slice(h * band, (h + 1) * band)
        total = jnp.concatenate([acc[0, n, mine, :] for n in range(2)], axis=1)
        local_mean = jnp.sum(total, axis=1, keepdims=True) * (1.0 / piece)
        gap = total - local_mean
        local_m2 = jnp.sum(gap * gap, axis=1, keepdims=True)
        st_out[h, 0:8, :] = jnp.broadcast_to(local_mean, (band, 128)).T[0:8, :]
        st_out[h, 8:16, :] = jnp.broadcast_to(local_m2, (band, 128)).T[0:8, :]
        for d in (1, 2, 3):
            stat_copy(h, d).start()

    def normalize(h):
        mine = slice(h * band, (h + 1) * band)
        for d in (1, 2, 3):
            stat_copy(h, d).wait_recv()
        means = [st_out[h, 0:8, :]] + [st_in[h, d, 0:8, :] for d in range(3)]
        m2s = [st_out[h, 8:16, :]] + [st_in[h, d, 8:16, :] for d in range(3)]
        mean = (means[0] + means[1] + means[2] + means[3]) * 0.25
        m2 = m2s[0] + m2s[1] + m2s[2] + m2s[3]
        for m in means:
            m2 += (m - mean) * (m - mean) * piece
        scale = lax.rsqrt(m2 * (1.0 / width) + norm_eps)
        mean_col = jnp.broadcast_to(mean[0:1, :], (128, band)).T[:, 0:1]
        scale_col = jnp.broadcast_to(scale[0:1, :], (128, band)).T[:, 0:1]
        for n in range(2):
            cut = slice(n * part_cols, (n + 1) * part_cols)
            out_ref[mine, cut] = (
                (acc[0, n, mine, :] - mean_col) * scale_col * gain_ref[:, cut]
                + bias_ref[:, cut]).astype(BF16)

    def last_settle(r, carry):
        settle(1, ranked(r))
        return carry
    lax.fori_loop(1, 2, last_settle, 0)
    collect_total(0)
    send_stats(0)
    give_own()
    lax.fori_loop(2, LAST - 1, last_settle, 0)

    @pl.when(inner == 0)
    def _():
        pair_copy(1).start()
    settle(1, ranked(LAST - 1))
    ret_copy(1, own).wait_recv()
    pair_copy(1).wait_recv()
    part[own, c, y, band_rows(1), :] += (
        core_in[own, y, band_rows(1), :] + y_in[own, band_rows(1), :] + pair_in[1])
    collect_total(1)
    send_stats(1)
    normalize(0)
    normalize(1)

    def sent_tokens(j, carry):
        for h in range(PASSES):
            y_copy(h, j).wait_send()
            z_copy(h, j).wait_send()
            for ch in (direct(j), swapped(j)):
                fwd_copy(h, ch).wait_send()
        return carry
    lax.fori_loop(0, HALF, sent_tokens, 0)
    for h in range(PASSES):
        for n in range(2):
            own_copy(h, n).wait_send()
    for k, e in enumerate(peers):
        meta_copy(e, k).wait_send()
    for n in range(2):
        pair_copy(n).wait_send()
    for h in range(PASSES):
        for i in range(PIECES):
            core_copy(h, i).wait_send()
        for d in (1, 2, 3):
            stat_copy(h, d).wait_send()
    for i in range(PIECES):
        ret_copy(0, i).wait_send()
        if i < SENT:
            scatter_copy(0, i).wait_send()
    for r in range(LAST + 1):
        ret_copy(1, ranked(r)).wait_send()
        if r < LAST - 1:
            scatter_copy(1, ranked(r)).wait_send()


def fused_on_device(tokens, expert_ids, gates, w_gate, w_up, w_down, norm_gain, norm_bias):
    rows, width = tokens.shape
    experts, _, hidden = w_gate.shape
    piece = norm_gain.shape[0]
    cols = width // CHUNKS
    part_cols = piece // 2
    band = rows // PASSES
    dma = pltpu.SemaphoreType.DMA
    vmem = pl.BlockSpec(memory_space=pltpu.VMEM)
    hbm = pl.BlockSpec(memory_space=pl.ANY)
    return pl.pallas_call(
        moe_kernel,
        out_shape=pltpu.VMEM((rows, piece), jnp.bfloat16),
        in_specs=[vmem] * 4 + [hbm] * 4,
        out_specs=vmem,
        scratch_shapes=[
            pltpu.VMEM((CHUNKS, 4, rows, cols), BF16),
            pltpu.VMEM((SLOTS, 2, experts, 2 * cols, hidden), BF16),
            pltpu.VMEM((PIECES, experts, hidden, part_cols), BF16),
            pltpu.VMEM((2, experts, 4 * CAP, hidden), F32),
            pltpu.VMEM((experts, 4 * CAP, hidden), BF16),
            pltpu.VMEM((experts, 4 * CAP, 2 * cols), BF16),
            pltpu.VMEM((4, experts * CAP, part_cols), BF16),
            pltpu.VMEM((PASSES, 4, experts * CAP, band), BF16),
            pltpu.VMEM((PASSES, 4, band, experts * CAP), BF16),
            pltpu.VMEM((PASSES, experts, 4 * CAP, 128), F32),
            pltpu.VMEM((4, 2 * experts, rows), F32),
            pltpu.VMEM((4, 2 * experts, rows), F32),
            pltpu.VMEM((PIECES, 2, 2, rows, part_cols), BF16),
            pltpu.VMEM((PIECES, 2, rows, part_cols), BF16),
            pltpu.VMEM((PIECES, rows, part_cols), BF16),
            pltpu.VMEM((PIECES, rows, part_cols), BF16),
            pltpu.VMEM((2, band, part_cols), BF16),
            pltpu.VMEM((PASSES, 16, band), F32),
            pltpu.VMEM((PASSES, 3, 16, band), F32),
            dma((CHUNKS,)), dma((PASSES, HALF)), dma((PASSES, HALF)),
            dma((PASSES, HALF)), dma((PASSES, HALF)),
            dma((PASSES, 2)), dma((PASSES, 2)), dma((PASSES, CHUNKS)), dma((PASSES, CHUNKS)),
            dma((3,)), dma((3,)), dma((SLOTS, 2)), dma((PIECES,)),
            dma((PASSES, PIECES)), dma((PASSES, PIECES)),
            dma((PASSES, PIECES)), dma((PASSES, PIECES)),
            dma((PASSES, PIECES)), dma((PASSES, PIECES)), dma((2,)), dma((2,)),
            dma((PASSES, 3)), dma((PASSES, 3)),
        ],
        compiler_params=pltpu.CompilerParams(
            collective_id=0, has_side_effects=True, vmem_limit_bytes=63 * 1024 * 1024),
    )(
        expert_ids.T, gates.T, norm_gain[None, :], norm_bias[None, :],
        tokens, w_gate, w_up, w_down,
    )


def solution(mesh):
    groups_apart = EXPERTS == GROUP_EXPERTS * mesh.shape["ep"]
    fused = groups_apart and mesh.shape["ep"] == 4 and mesh.shape["tp"] == 4
    return jax.shard_map(
        fused_on_device if fused else on_device,
        mesh=mesh,
        in_specs=(
            P(("grp", "ep"), None),
            P(("grp", "ep"), None),
            P(("grp", "ep"), None),
            P("ep", None, "tp"),
            P("ep", None, "tp"),
            P("ep", "tp", None),
            P("tp"),
            P("tp"),
        ),
        out_specs=P(("grp", "ep"), "tp"),
        check_vma=False,
    )
```

```python
import functools
import jax
import jax.numpy as jnp
from jax import lax
from jax.experimental import pallas as pl
from jax.experimental.pallas import tpu as pltpu
from jax.sharding import PartitionSpec as P

D = 4096
TOPK = 2
EXPERTS = 16
CAP = 64


norm_eps = 1e-05


def route_slots(expert_ids):
    flat_ids = expert_ids.reshape(-1)
    onehot = (flat_ids[:, None] == jnp.arange(EXPERTS, dtype=jnp.int32)[None, :]).astype(jnp.int32)
    position = jnp.sum((jnp.cumsum(onehot, axis=0) - 1) * onehot, axis=1)
    target = flat_ids * CAP + position
    token_of = jnp.arange(flat_ids.shape[0], dtype=jnp.int32) // TOPK
    source = jnp.zeros((EXPERTS * CAP,), jnp.int32).at[target].set(token_of)
    filled = jnp.zeros((EXPERTS * CAP,), jnp.bool_).at[target].set(True)
    return (target, source, filled)


def on_device(tokens, expert_ids, gates, w_gate, w_up, w_down, norm_gain, norm_bias):
    tok_rows, width = tokens.shape
    piece_width = norm_gain.shape[0]
    target, source, filled = route_slots(expert_ids)
    outgoing = jnp.where(filled[:, None], tokens[source], jnp.zeros((), jnp.bfloat16)).reshape(
        EXPERTS, CAP, width
    )
    arrived = lax.all_to_all(outgoing, "ep", split_axis=0, concat_axis=1, tiled=True)
    gate_part = jnp.einsum("erd,edf->erf", arrived, w_gate, preferred_element_type=jnp.float32)
    up_part = jnp.einsum("erd,edf->erf", arrived, w_up, preferred_element_type=jnp.float32)
    hidden = (jax.nn.silu(gate_part) * up_part).astype(jnp.bfloat16)
    partial_value = jnp.einsum("erf,efd->erd", hidden, w_down, preferred_element_type=jnp.float32)
    summed = lax.psum_scatter(
        partial_value.astype(jnp.bfloat16), "tp", scatter_dimension=2, tiled=True
    )
    returned = lax.all_to_all(summed, "ep", split_axis=1, concat_axis=0, tiled=True)
    picked = returned.reshape(EXPERTS * CAP, piece_width)[target].reshape(
        tok_rows, TOPK, piece_width
    )
    combined = jnp.sum(picked.astype(jnp.float32) * gates[:, :, None], axis=1)
    stats = lax.psum((jnp.sum(combined, axis=1), jnp.sum(combined * combined, axis=1)), "tp")
    row_mean = stats[0] / D
    row_var = stats[1] / D - row_mean * row_mean
    normed = (combined - row_mean[:, None]) * lax.rsqrt(
        row_var[:, None] + norm_eps
    ) * norm_gain + norm_bias
    return normed.astype(jnp.bfloat16)


GROUP_EXPERTS = 4
CHUNKS = 16
HALF = CHUNKS // 2
PASSES = 2
SLOTS = 3
PIECES = 8
SENT = 6
FIRST_RELAYS = (
    ((0, 1), ()), ((2, 3), (0, 1)), ((4, 5), ()), ((6,), (2, 3)),
    ((7,), ()), ((8,), (4, 5)), ((9,), (6, 7)), ((10, 11, 12), (8,)),
)
SECOND_RELAYS = (
    ((13, 14, 15), (9, 10)), ((), (11,)), ((), (12, 13)), ((), (14, 15)),
    ((), ()), ((), ()), ((), ()), ((), ()),
)
SECOND_PIECES = (
    ((0, 1), (), ()), ((2,), (), ()), ((3,), (0,), (0,)), ((4,), (1,), (1,)),
    ((5,), (2,), ()), ((6,), (3,), (2,)), ((7,), (4,), (3,)), ((), (), (4,)),
)
LATE_SETTLES = ((4, 6), (6, 7))
LAST = 6
F32 = jnp.float32
BF16 = jnp.bfloat16
MESH = pl.DeviceIdType.MESH


def moe_kernel(
    ids_ref, gates_ref, gain_ref, bias_ref, tokens_ref, wg_ref, wu_ref, wd_ref,
    out_ref,
    tok, wbuf, wd, acc, hid, xr, dnb, place, collect, rowg, meta, meta_in,
    part, core_in, y_in, z_in, pair_in, st_out, st_in,
    tok_sem, y_send, y_recv, z_send, z_recv, own_send, own_recv, fwd_send, fwd_recv,
    meta_send, meta_recv, w_sem, wd_sem, pc_send, pc_recv, py_send, py_recv,
    pz_send, pz_recv, pair_send, pair_recv, st_send, st_recv,
):
    ep = lax.axis_index("ep")
    z = lax.axis_index("tp")
    y, c = ep // 2, ep % 2
    partner = y * 2 + (1 - c)
    across = (1 - y) * 2 + c
    diag = (1 - y) * 2 + (1 - c)
    par, side = z % 2, z // 2
    zpeer = z + 1 - 2 * par
    rows, width = tokens_ref.shape
    band = rows // PASSES
    experts = wg_ref.shape[0]
    cols = width // CHUNKS
    piece = gain_ref.shape[1]
    part_cols = piece // 2

    def remote(src, dst, send, recv, e, t):
        return pltpu.make_async_remote_copy(
            src_ref=src, dst_ref=dst, send_sem=send, recv_sem=recv,
            device_id={"ep": e, "tp": t}, device_id_type=MESH,
        )

    def span(ch, size):
        return pl.ds(pl.multiple_of(ch * size, size), size)

    def load_tok(ch):
        return pltpu.make_async_copy(
            tokens_ref.at[:, span(ch, cols)], tok.at[ch, ep], tok_sem.at[ch])

    def band_rows(h):
        return pl.ds(pl.multiple_of(h * band, band), band)

    inner = par + side - 2 * par * side
    paired = 5 - 4 * inner
    own = PIECES - 1

    def flip(far, near):
        return 2 * (side + far - 2 * side * far) + par + near - 2 * par * near

    def target(i):
        mask = (1 - inner) * (3 - i // 2) + inner * ((i // 2 + 1) % 4)
        return flip(mask // 2, mask % 2)

    def ranked(r):
        return r + (1 - inner) * (r // 5) + inner * ((r + 6) // 7)

    def load_wd(i):
        return pltpu.make_async_copy(
            wd_ref.at[:, :, span(target(i) * 2 + i % 2, part_cols)], wd.at[i], wd_sem.at[i])

    def direct(j):
        return par * HALF + j

    def swapped(j):
        return (1 - par) * HALF + j

    def unit_chunk(u):
        late, begun = u // 7, (u + 7) // 8
        kind = (1 - u % 2) * begun + late
        index = (u + 1) // 2 - (1 - u % 2) * begun - late
        return (par + kind - 2 * par * kind) * HALF + 2 * index

    def load_unit(t):
        first = unit_chunk(t % HALF)
        window = pl.ds(pl.multiple_of(first * cols, 2 * cols), 2 * cols)
        return [
            pltpu.make_async_copy(
                w_ref.at[:, window, :], wbuf.at[t % SLOTS, g], w_sem.at[t % SLOTS, g])
            for g, w_ref in enumerate((wg_ref, wu_ref))
        ]

    def y_copy(h, j):
        blk = tok.at[direct(j), ep, band_rows(h)]
        return remote(blk, blk, y_send.at[h, j], y_recv.at[h, j], across, z)

    def y_arrive(h, j):
        blk = tok.at[direct(j), across, band_rows(h)]
        return remote(blk, blk, y_send.at[h, j], y_recv.at[h, j], across, z)

    def z_copy(h, j):
        blk = tok.at[direct(j), across, band_rows(h)]
        return remote(blk, blk, z_send.at[h, j], z_recv.at[h, j], ep, zpeer)

    def z_arrive(h, j):
        blk = tok.at[swapped(j), across, band_rows(h)]
        return remote(blk, blk, z_send.at[h, j], z_recv.at[h, j], ep, zpeer)

    def own_copy(h, n):
        blk = tok.at[pl.ds(n * HALF, HALF), ep, band_rows(h)]
        return remote(blk, blk, own_send.at[h, n], own_recv.at[h, n], partner, z)

    def own_arrive(h, n):
        blk = tok.at[pl.ds(n * HALF, HALF), partner, band_rows(h)]
        return remote(blk, blk, own_send.at[h, n], own_recv.at[h, n], partner, z)

    def fwd_copy(h, ch):
        blk = tok.at[ch, across, band_rows(h)]
        return remote(blk, blk, fwd_send.at[h, ch], fwd_recv.at[h, ch], partner, z)

    def fwd_arrive(h, ch):
        blk = tok.at[ch, diag, band_rows(h)]
        return remote(blk, blk, fwd_send.at[h, ch], fwd_recv.at[h, ch], partner, z)

    def meta_copy(e, k):
        return remote(meta.at[e], meta_in.at[ep], meta_send.at[k], meta_recv.at[k], e, z)

    def meta_arrive(e, k):
        return remote(meta.at[e], meta_in.at[e], meta_send.at[k], meta_recv.at[k], e, z)

    peers = (partner, across, diag)

    for j in range(HALF):
        load_tok(direct(j)).start()
    for j in range(HALF):
        load_tok(swapped(j)).start()

    barrier = pltpu.get_barrier_semaphore()
    for e in peers:
        pl.semaphore_signal(barrier, inc=1, device_id={"ep": e, "tp": z}, device_id_type=MESH)
    for d in (1, 2, 3):
        pl.semaphore_signal(
            barrier, inc=1, device_id={"ep": ep, "tp": (z + d) % 4}, device_id_type=MESH)
    total_experts = 4 * experts
    expert_row = lax.broadcasted_iota(jnp.int32, (total_experts, rows), 0)
    first = ids_ref[0:1, :] == expert_row
    second = ids_ref[1:2, :] == expert_row
    named = jnp.where(first | second, 1.0, 0.0).astype(F32)
    weight = jnp.where(first, gates_ref[0:1, :], jnp.where(second, gates_ref[1:2, :], 0.0))
    tri_r = lax.broadcasted_iota(jnp.int32, (rows, rows), 0)
    tri_c = lax.broadcasted_iota(jnp.int32, (rows, rows), 1)
    before = jnp.where(
        (tri_r < tri_c) & (tri_r // band == tri_c // band), 1.0, 0.0).astype(BF16)
    position = jnp.dot(named.astype(BF16), before, preferred_element_type=F32)
    slot = jnp.where(
        named > 0.5, position + ((expert_row % experts) * CAP).astype(F32), -1.0)
    for e in range(4):
        meta[e, 0:experts, :] = slot[e * experts:(e + 1) * experts, :]
        meta[e, experts:2 * experts, :] = weight[e * experts:(e + 1) * experts, :]
    for ch in range(CHUNKS):
        load_tok(ch).wait()
    for t in range(SLOTS):
        for cp in load_unit(t):
            cp.start()
    for i in range(PIECES):
        load_wd(i).start()
    pl.semaphore_wait(barrier, 6)
    for k, e in enumerate(peers):
        meta_copy(e, k).start()
    for h in range(PASSES):
        for j in range(HALF):
            y_copy(h, j).start()
        for n in range(2):
            own_copy(h, n).start()

    meta_in[ep] = meta[ep]
    for k, e in enumerate(peers):
        meta_arrive(e, k).wait_recv()
    for n in range(2):
        own_arrive(0, n).wait_recv()

    row_f = tri_r.astype(F32)
    for s in range(4):
        info = meta_in[s]
        put = jnp.zeros((rows, rows), F32)
        for e in range(experts):
            put += jnp.where(row_f == info[e:e + 1, :], 1.0, 0.0)
        back = put.T
        for h in range(PASSES):
            mine = slice(h * band, (h + 1) * band)
            place[h, s] = put[:, mine].astype(BF16)
            collect[h, s] = back[mine, :].astype(BF16)
            for e in range(experts):
                g = jnp.sum(
                    put[e * CAP:(e + 1) * CAP, mine]
                    * info[experts + e:experts + e + 1, mine],
                    axis=1, keepdims=True)
                rowg[h, e, s * CAP:(s + 1) * CAP, :] = jnp.broadcast_to(g, (CAP, 128))

    def unit(h, u):
        t = h * HALF + u
        chunks = [unit_chunk(u) + k for k in range(2)]
        for ch in chunks:
            fwd_arrive(h, ch).wait_recv()
        for cp in load_unit(t):
            cp.wait()
        for k, ch in enumerate(chunks):
            for s in range(4):
                x = jnp.dot(
                    place[h, s], tok[ch, s, band_rows(h), :],
                    preferred_element_type=F32).astype(BF16)
                for e in range(experts):
                    xr[e, s * CAP:(s + 1) * CAP, k * cols:(k + 1) * cols] = (
                        x[e * CAP:(e + 1) * CAP, :])
        for e in range(experts):
            for g in range(2):
                product = jnp.dot(xr[e], wbuf[t % SLOTS, g, e], preferred_element_type=F32)
                acc[g, e] = product if u == 0 else acc[g, e] + product

        if t + SLOTS < PASSES * HALF:
            for cp in load_unit(t + SLOTS):
                cp.start()

    def relay_y(r):
        h, j = r // HALF, r % HALF
        y_arrive(h, j).wait_recv()
        z_copy(h, j).start()
        fwd_copy(h, direct(j)).start()

    def relay_z(r):
        h, j = r // HALF, r % HALF
        z_arrive(h, j).wait_recv()
        fwd_copy(h, swapped(j)).start()

    def relay(ys, zs):
        for r in ys:
            relay_y(r)
        for r in zs:
            relay_z(r)

    def activate(h):
        def one(e, carry):
            g = acc[0, e]
            v = g / (1.0 + jnp.exp(-g)) * acc[1, e]
            hid[e] = (v * rowg[h, e][:, 0:1]).astype(BF16)
            return carry
        lax.fori_loop(0, experts, one, 0)

    def core_copy(h, i):
        return remote(
            part.at[i, 1 - c, :, band_rows(h)], core_in.at[i, :, band_rows(h)],
            pc_send.at[h, i], pc_recv.at[h, i], partner, z)

    def ret_copy(h, i):
        return remote(
            part.at[i, c, 1 - y, band_rows(h)], y_in.at[i, band_rows(h)],
            py_send.at[h, i], py_recv.at[h, i], across, z)

    def scatter_slot(h, slot, i, dest):
        return remote(
            part.at[i, c, y, band_rows(h)], z_in.at[slot, band_rows(h)],
            pz_send.at[h, slot], pz_recv.at[h, slot], ep, dest)

    def scatter_copy(h, i):
        onward = inner * ((i + 6) // 8)
        return scatter_slot(
            h, i + 2 * inner * (i // 4), i, zpeer + onward * (target(i) - zpeer))

    def scattered(h, slot):
        return scatter_slot(h, slot, 0, zpeer)

    def down(h, i):
        if h == 0:
            load_wd(i).wait()

        for e in range(experts):
            o = jnp.dot(hid[e], wd[i, e], preferred_element_type=F32).astype(BF16)
            for s in range(4):
                dnb[s, e * CAP:(e + 1) * CAP, :] = o[s * CAP:(s + 1) * CAP, :]
        for s in range(4):
            part[i, s % 2, s // 2, band_rows(h), :] = jnp.dot(
                collect[h, s], dnb[s], preferred_element_type=F32).astype(BF16)
        core_copy(h, i).start()

    def pair_copy(n):
        return remote(
            part.at[paired, c, (1 - y) + n * (2 * y - 1), band_rows(1)], pair_in.at[n],
            pair_send.at[n], pair_recv.at[n], ep, zpeer)

    def give_pair():
        core_copy(1, paired).wait_recv()
        part[paired, c, :, band_rows(1), :] += core_in[paired, :, band_rows(1), :]
        pair_copy(0).start()

        @pl.when(inner == 1)
        def _():
            pair_copy(1).start()

    def give_own():
        core_copy(1, own).wait_recv()
        pair_copy(0).wait_recv()
        part[own, c, 1 - y, band_rows(1), :] += (
            core_in[own, 1 - y, band_rows(1), :] + pair_in[0])
        ret_copy(1, own).start()

    def give_back(h, i):
        core_copy(h, i).wait_recv()
        part[i, c, 1 - y, band_rows(h), :] += core_in[i, 1 - y, band_rows(h), :]
        ret_copy(h, i).start()

    def settle(h, i):
        ret_copy(h, i).wait_recv()
        part[i, c, y, band_rows(h), :] += (
            core_in[i, y, band_rows(h), :] + y_in[i, band_rows(h), :])

        @pl.when((inner == 1) & (i >= 2) & (i < SENT))
        def _():
            scattered(h, i - 2).wait_recv()
            part[i, c, y, band_rows(h), :] += z_in[i - 2, band_rows(h), :]

        @pl.when(i < SENT)
        def _():
            scatter_copy(h, i).start()

    for u in range(HALF):
        relay(*FIRST_RELAYS[u])
        unit(0, u)
    activate(0)
    for n in range(2):
        own_arrive(1, n).wait_recv()

    for u in range(HALF):
        downs, outer_settles, inner_settles = SECOND_PIECES[u]
        for i in downs:
            down(0, i)
        if u == 0:
            give_back(0, 0)
        relay(*SECOND_RELAYS[u])
        unit(1, u)
        for i in downs:
            if i != 0:
                give_back(0, i)
        for v, settles in enumerate((outer_settles, inner_settles)):
            for i in settles:
                @pl.when(inner == v)
                def _():
                    settle(0, i)
    activate(1)

    def nth(n):
        second = (8 - n) // 7 - (7 - n) // 7
        r = n - (n + 6) // 8
        return second * paired + (1 - second) * ranked(r)

    def last_down(n, carry):
        @pl.when(n < PIECES)
        def _():
            down(1, nth(n))

        @pl.when(n == 2)
        def _():
            give_pair()

        @pl.when((n >= 1) & (n != 2))
        def _():
            give_back(1, nth(n - 1))
        for step, i in LATE_SETTLES:
            @pl.when(n == step)
            def _():
                settle(0, i)

        @pl.when(n == inner)
        def _():
            settle(0, SENT - 1)

        @pl.when(n == 6 + inner)
        def _():
            settle(1, ranked(0))
        return carry
    lax.fori_loop(0, PIECES, last_down, 0)

    def stat_copy(h, d):
        return remote(
            st_out.at[h], st_in.at[h, d - 1],
            st_send.at[h, d - 1], st_recv.at[h, d - 1], ep, (z + d) % 4)

    def collect_total(h):
        for n in range(2):
            half = part[SENT + n, c, y, band_rows(h), :].astype(F32)
            for k in (n, 2 + n) if h == 0 or n == 0 else (2 + n,):
                slot = 4 * inner + k
                scattered(h, slot).wait_recv()
                half += z_in[slot, band_rows(h), :].astype(F32)
            acc[0, n, h * band:(h + 1) * band, :] = half

    def send_stats(h):
        mine = slice(h * band, (h + 1) * band)
        total = jnp.concatenate([acc[0, n, mine, :] for n in range(2)], axis=1)
        local_mean = jnp.sum(total, axis=1, keepdims=True) * (1.0 / piece)
        gap = total - local_mean
        local_m2 = jnp.sum(gap * gap, axis=1, keepdims=True)
        st_out[h, 0:8, :] = jnp.broadcast_to(local_mean, (band, 128)).T[0:8, :]
        st_out[h, 8:16, :] = jnp.broadcast_to(local_m2, (band, 128)).T[0:8, :]
        for d in (1, 2, 3):
            stat_copy(h, d).start()

    def normalize(h):
        mine = slice(h * band, (h + 1) * band)
        for d in (1, 2, 3):
            stat_copy(h, d).wait_recv()
        means = [st_out[h, 0:8, :]] + [st_in[h, d, 0:8, :] for d in range(3)]
        m2s = [st_out[h, 8:16, :]] + [st_in[h, d, 8:16, :] for d in range(3)]
        mean = (means[0] + means[1] + means[2] + means[3]) * 0.25
        m2 = m2s[0] + m2s[1] + m2s[2] + m2s[3]
        for m in means:
            m2 += (m - mean) * (m - mean) * piece
        scale = lax.rsqrt(m2 * (1.0 / width) + norm_eps)
        mean_col = jnp.broadcast_to(mean[0:1, :], (128, band)).T[:, 0:1]
        scale_col = jnp.broadcast_to(scale[0:1, :], (128, band)).T[:, 0:1]
        for n in range(2):
            cut = slice(n * part_cols, (n + 1) * part_cols)
            out_ref[mine, cut] = (
                (acc[0, n, mine, :] - mean_col) * scale_col * gain_ref[:, cut]
                + bias_ref[:, cut]).astype(BF16)

    def last_settle(r, carry):
        settle(1, ranked(r))
        return carry
    lax.fori_loop(1, 2, last_settle, 0)
    collect_total(0)
    send_stats(0)
    give_own()
    lax.fori_loop(2, LAST - 2, last_settle, 0)

    @pl.when(inner == 0)
    def _():
        pair_copy(1).start()
    settle(1, ranked(LAST - 2))
    settle(1, ranked(LAST - 1))
    ret_copy(1, own).wait_recv()
    pair_copy(1).wait_recv()
    part[own, c, y, band_rows(1), :] += (
        core_in[own, y, band_rows(1), :] + y_in[own, band_rows(1), :] + pair_in[1])
    collect_total(1)
    send_stats(1)
    normalize(0)
    normalize(1)

    def sent_tokens(j, carry):
        for h in range(PASSES):
            y_copy(h, j).wait_send()
            z_copy(h, j).wait_send()
            for ch in (direct(j), swapped(j)):
                fwd_copy(h, ch).wait_send()
        return carry
    lax.fori_loop(0, HALF, sent_tokens, 0)
    for h in range(PASSES):
        for n in range(2):
            own_copy(h, n).wait_send()
    for k, e in enumerate(peers):
        meta_copy(e, k).wait_send()
    for n in range(2):
        pair_copy(n).wait_send()
    for h in range(PASSES):
        for i in range(PIECES):
            core_copy(h, i).wait_send()
        for d in (1, 2, 3):
            stat_copy(h, d).wait_send()
    for i in range(PIECES):
        ret_copy(0, i).wait_send()
        if i < SENT:
            scatter_copy(0, i).wait_send()
    for r in range(LAST + 1):
        ret_copy(1, ranked(r)).wait_send()
        if r < LAST - 1:
            scatter_copy(1, ranked(r)).wait_send()


def fused_on_device(tokens, expert_ids, gates, w_gate, w_up, w_down, norm_gain, norm_bias):
    rows, width = tokens.shape
    experts, _, hidden = w_gate.shape
    piece = norm_gain.shape[0]
    cols = width // CHUNKS
    part_cols = piece // 2
    band = rows // PASSES
    dma = pltpu.SemaphoreType.DMA
    vmem = pl.BlockSpec(memory_space=pltpu.VMEM)
    hbm = pl.BlockSpec(memory_space=pl.ANY)
    return pl.pallas_call(
        moe_kernel,
        out_shape=pltpu.VMEM((rows, piece), jnp.bfloat16),
        in_specs=[vmem] * 4 + [hbm] * 4,
        out_specs=vmem,
        scratch_shapes=[
            pltpu.VMEM((CHUNKS, 4, rows, cols), BF16),
            pltpu.VMEM((SLOTS, 2, experts, 2 * cols, hidden), BF16),
            pltpu.VMEM((PIECES, experts, hidden, part_cols), BF16),
            pltpu.VMEM((2, experts, 4 * CAP, hidden), F32),
            pltpu.VMEM((experts, 4 * CAP, hidden), BF16),
            pltpu.VMEM((experts, 4 * CAP, 2 * cols), BF16),
            pltpu.VMEM((4, experts * CAP, part_cols), BF16),
            pltpu.VMEM((PASSES, 4, experts * CAP, band), BF16),
            pltpu.VMEM((PASSES, 4, band, experts * CAP), BF16),
            pltpu.VMEM((PASSES, experts, 4 * CAP, 128), F32),
            pltpu.VMEM((4, 2 * experts, rows), F32),
            pltpu.VMEM((4, 2 * experts, rows), F32),
            pltpu.VMEM((PIECES, 2, 2, rows, part_cols), BF16),
            pltpu.VMEM((PIECES, 2, rows, part_cols), BF16),
            pltpu.VMEM((PIECES, rows, part_cols), BF16),
            pltpu.VMEM((PIECES, rows, part_cols), BF16),
            pltpu.VMEM((2, band, part_cols), BF16),
            pltpu.VMEM((PASSES, 16, band), F32),
            pltpu.VMEM((PASSES, 3, 16, band), F32),
            dma((CHUNKS,)), dma((PASSES, HALF)), dma((PASSES, HALF)),
            dma((PASSES, HALF)), dma((PASSES, HALF)),
            dma((PASSES, 2)), dma((PASSES, 2)), dma((PASSES, CHUNKS)), dma((PASSES, CHUNKS)),
            dma((3,)), dma((3,)), dma((SLOTS, 2)), dma((PIECES,)),
            dma((PASSES, PIECES)), dma((PASSES, PIECES)),
            dma((PASSES, PIECES)), dma((PASSES, PIECES)),
            dma((PASSES, PIECES)), dma((PASSES, PIECES)), dma((2,)), dma((2,)),
            dma((PASSES, 3)), dma((PASSES, 3)),
        ],
        compiler_params=pltpu.CompilerParams(
            collective_id=0, has_side_effects=True, vmem_limit_bytes=63 * 1024 * 1024),
    )(
        expert_ids.T, gates.T, norm_gain[None, :], norm_bias[None, :],
        tokens, w_gate, w_up, w_down,
    )


def solution(mesh):
    groups_apart = EXPERTS == GROUP_EXPERTS * mesh.shape["ep"]
    fused = groups_apart and mesh.shape["ep"] == 4 and mesh.shape["tp"] == 4
    return jax.shard_map(
        fused_on_device if fused else on_device,
        mesh=mesh,
        in_specs=(
            P(("grp", "ep"), None),
            P(("grp", "ep"), None),
            P(("grp", "ep"), None),
            P("ep", None, "tp"),
            P("ep", None, "tp"),
            P("ep", "tp", None),
            P("tp"),
            P("tp"),
        ),
        out_specs=P(("grp", "ep"), "tp"),
        check_vma=False,
    )
```
